32 devices in a mesh: ep: 32 (over z, y, x, core).
Axes of the slice: x: 2, y: 2, z: 4, core: 2. Of those that a mesh axis runs over, the one named last changes fastest.
Arguments:
- tokens: bfloat16 [384, 2048], P('ep'), may hold values from -6 to 6
- cache_latent: bfloat16 [384, 1024, 512], P('ep'), may hold values from -180 to 180
- cache_rope: bfloat16 [384, 1024, 64], P('ep'), may hold values from -6 to 6
- cache_lengths: int32 [384], P('ep'), may hold values from 1 to 1024, as said below
- expert_ids: int32 [384, 6], P('ep'), may hold values from 0 to 15, as said below
- route_weight: float32 [384, 6], P('ep'), may hold values from 1 to 2
- attn_gain: float32 [2048], replicated, may hold values from 0.1 to 1.9
- q_gain: float32 [512], replicated, may hold values from 0.1 to 1.9
- kv_gain: float32 [512], replicated, may hold values from 0.1 to 1.9
- moe_gain: float32 [2048], replicated, may hold values from 0.1 to 1.9
- w_qdown: bfloat16 [2048, 512], replicated, may hold values from -0.125 to 0.125
- w_kvdown: bfloat16 [2048, 512], replicated, may hold values from -0.125 to 0.125
- w_krope: bfloat16 [2048, 64], replicated, may hold values from -0.125 to 0.125
- w_qup: bfloat16 [512, 1536], replicated, may hold values from -0.25 to 0.25
- w_kup: bfloat16 [512, 1024], replicated, may hold values from -0.5 to 0.5
- w_vup: bfloat16 [512, 1024], replicated, may hold values from -0.25 to 0.25
- w_out: bfloat16 [1024, 2048], replicated, may hold values from -0.1875 to 0.1875
- expert_gate: bfloat16 [32, 2048, 256], P('ep'), may hold values from -0.125 to 0.125
- expert_up: bfloat16 [32, 2048, 256], P('ep'), may hold values from -0.125 to 0.125
- expert_down: bfloat16 [32, 256, 2048], P('ep'), may hold values from -0.25 to 0.25
Outputs:
- mixed: float32 [384, 2048], P('ep')
- new_latent: bfloat16 [384, 512], P('ep')
- new_rope_key: bfloat16 [384, 64], P('ep')
The draws below stay inside these ranges and needn't reach their ends.
Inputs may be any that keep to these rules, and one draw needn't show every extreme that they name: `cache_lengths`: some sequence holds 1024 positions. `expert_ids`: each row names 6 different experts of one group g, numbered g * 16 to g * 16 + 15; among the rows of one device no expert is named more than 5 times, and some expert exactly 5 times.
All inputs are finite; a program needn't handle non-finite values.
Results may differ from the reference program's by a relative error of at most 0.03.
Values may be sent and summed in bfloat16 or wider, within the bound.
No kernel may reach another device: no remote copies, remote signals or barrier semaphores. Data moves between devices by JAX's collectives and lax.ppermute only.
A program may use at most 128 MiB of HBM per device.

```python
import jax
import jax.numpy as jnp
from jax import lax

D = 2048
HEADS = 8
Q_RANK = 512
KV_RANK = 512
NOPE_DIM = 128
ROPE_DIM = 64
VALUE_DIM = 128
FF = 512
GROUP_SIZE = 16
TOP_K = 6
SEQ_DEV = 12
CACHE = 1024
TOKENS = 384
EXPERTS = 16
GROUPS = 1
GROUP_MOST = 12
CAPACITY = 5
N_EP = 32


def draw_cache_lengths(key, part):
    block_count = TOKENS // SEQ_DEV
    key_list = jax.random.split(jax.random.fold_in(key, 7), 2)
    factor = jax.random.randint(key_list[0], (block_count, 1), 1, 5)
    upper_bound = CACHE * factor // 4
    raw_bits = jax.random.randint(key_list[1], (block_count, SEQ_DEV), 0, 1 << 30)
    lengths = (1 + raw_bits % upper_bound).reshape(TOKENS)
    lengths = lengths.at[0].set(CACHE)
    return lengths.astype(jnp.int32)


def draw_expert_ids(key, part):
    block_count = TOKENS // SEQ_DEV
    base_key = jax.random.fold_in(key, 13)
    seq_order = jax.vmap(lambda sub_key: jax.random.permutation(sub_key, SEQ_DEV))(jax.random.split(jax.random.fold_in(base_key, 1), block_count))
    group_order = jax.vmap(lambda sub_key: jax.random.permutation(sub_key, GROUPS))(jax.random.split(jax.random.fold_in(base_key, 2), block_count))
    local_table = jax.vmap(lambda sub_key: jax.random.permutation(sub_key, GROUP_SIZE))(jax.random.split(jax.random.fold_in(base_key, 3), block_count * GROUPS)).reshape(block_count, GROUPS, GROUP_SIZE)
    others = max(GROUPS - 1, 1)
    first_run = seq_order < GROUP_MOST
    rest_rank = jnp.maximum(seq_order - GROUP_MOST, 0)
    slot_index = jnp.where(first_run, 0, 1 + rest_rank % others)
    group_rank = jnp.where(first_run, seq_order, rest_rank // others)
    group_ids = jnp.take_along_axis(group_order, slot_index, axis=1)
    spot_index = (group_rank[:, :, None] * TOP_K + jnp.arange(TOP_K, dtype=jnp.int32)[None, None, :]) % GROUP_SIZE
    chosen_tables = local_table[jnp.arange(block_count)[:, None], group_ids]
    local_ids = jnp.take_along_axis(chosen_tables, spot_index, axis=2)
    return (group_ids[:, :, None] * GROUP_SIZE + local_ids).reshape(TOKENS, TOP_K).astype(jnp.int32)


def draw_cache_latent(key, part):
    key_list = jax.random.split(jax.random.fold_in(key, 17), 1)
    values = jnp.clip(jax.random.normal(key_list[0], (TOKENS, CACHE, KV_RANK), jnp.float32), -6.0, 6.0)
    return values.astype(jnp.bfloat16)


def block_levels(key, dims, cuts, least, high):
    loudness = 1.0
    for axis_at, shards_of in cuts:
        steps = jax.random.uniform(jax.random.fold_in(jax.random.fold_in(key, 6), axis_at), (shards_of,), jnp.float32, least / len(cuts), high / len(cuts))
        loudness = loudness * jnp.repeat(jnp.exp(steps), dims[axis_at] // shards_of).reshape((-1,) + (1,) * (len(dims) - 1 - axis_at))
    return loudness


def scatter_about(rng, shape, deviation, limit, cuts=(), held_as=jnp.bfloat16):
    values = jax.random.normal(rng, shape, jnp.float32) * deviation
    if len(cuts) > 0:
        values = block_levels(rng, shape, cuts, -0.22, 0.18) * values
    return jnp.clip(values, min=-limit, max=limit).astype(held_as)


def setup_inputs(seed: int = 0) -> dict:
    arg_keys = jax.random.split(jax.random.key(seed), 21)
    return {
        "tokens": scatter_about(arg_keys[0], (TOKENS, D), 1.0, 6.0, ((0, 32),)),
        "cache_latent": draw_cache_latent(jax.random.fold_in(arg_keys[20], 71), 0),
        "cache_rope": scatter_about(arg_keys[2], (TOKENS, CACHE, ROPE_DIM), 1.0, 6.0, ((0, 32),)),
        "cache_lengths": draw_cache_lengths(jax.random.fold_in(arg_keys[20], 71), 0),
        "expert_ids": draw_expert_ids(jax.random.fold_in(arg_keys[20], 71), 0),
        "route_weight": jnp.clip(1.0 + 1.0 * jax.random.uniform(arg_keys[5], (TOKENS, TOP_K), jnp.float32) ** block_levels(arg_keys[5], (TOKENS, TOP_K), ((0, 32),), -0.2, 0.2), 1.0, 2.0),
        "attn_gain": jnp.clip(1.0 + 0.18 * jax.random.normal(arg_keys[6], (D,), jnp.float32), 0.1, 1.9),
        "q_gain": jnp.clip(1.0 + 0.18 * jax.random.normal(arg_keys[7], (Q_RANK,), jnp.float32), 0.1, 1.9),
        "kv_gain": jnp.clip(1.0 + 0.18 * jax.random.normal(arg_keys[8], (KV_RANK,), jnp.float32), 0.1, 1.9),
        "moe_gain": jnp.clip(1.0 + 0.18 * jax.random.normal(arg_keys[9], (D,), jnp.float32), 0.1, 1.9),
        "w_qdown": scatter_about(arg_keys[10], (D, Q_RANK), D ** -0.5, 0.125),
        "w_kvdown": scatter_about(arg_keys[11], (D, KV_RANK), D ** -0.5, 0.125),
        "w_krope": scatter_about(arg_keys[12], (D, ROPE_DIM), D ** -0.5, 0.125),
        "w_qup": scatter_about(arg_keys[13], (Q_RANK, HEADS * (NOPE_DIM + ROPE_DIM)), Q_RANK ** -0.5, 0.25),
        "w_kup": scatter_about(arg_keys[14], (KV_RANK, HEADS * NOPE_DIM), NOPE_DIM ** -0.5, 0.5),
        "w_vup": scatter_about(arg_keys[15], (KV_RANK, HEADS * VALUE_DIM), KV_RANK ** -0.5, 0.25),
        "w_out": scatter_about(arg_keys[16], (HEADS * VALUE_DIM, D), (HEADS * VALUE_DIM) ** -0.5, 0.1875),
        "expert_gate": scatter_about(arg_keys[17], (EXPERTS * 2, D, FF // 2), D ** -0.5, 0.125, ((0, 32),)),
        "expert_up": scatter_about(arg_keys[18], (EXPERTS * 2, D, FF // 2), D ** -0.5, 0.125, ((0, 32),)),
        "expert_down": scatter_about(arg_keys[19], (EXPERTS * 2, FF // 2, D), FF ** -0.5, 0.25, ((0, 32),)),
    }


EPS = 1e-06
THETA = 10000.0

def norm_gain(values, gain_vec):
    values = values.astype(jnp.float32)
    return values * lax.rsqrt(lax.optimization_barrier(jnp.mean(values * values, axis=-1, keepdims=True)) + EPS) * gain_vec.astype(jnp.float32)

def rotary_angles(lengths):
    half_width = ROPE_DIM // 2
    inverse = THETA ** (-jnp.arange(half_width, dtype=jnp.float32) / half_width)
    return lengths.astype(jnp.float32)[:, None] * inverse[None, :]

def rotate(values, angles):
    half_width = values.shape[-1] // 2
    first_half = values[..., :half_width]
    second = values[..., half_width:]
    cosine = jnp.cos(angles)
    sine_part = jnp.sin(angles)
    return jnp.concatenate([first_half * cosine - second * sine_part, second * cosine + first_half * sine_part], axis=-1)

def routed(moe_in, expert_ids, route_weight, expert_gate, expert_up, expert_down):
    row_count = moe_in.shape[0]
    most_rows = N_EP * CAPACITY
    padded = jnp.concatenate([moe_in, jnp.zeros((1, D), moe_in.dtype)], axis=0)

    def one_half(running, inputs):
        half_index, gate_half, up_half, down_half = inputs
        expert = half_index // 2
        match_mask = expert_ids == expert
        weight_sum = lax.optimization_barrier(jnp.sum(jnp.where(match_mask, route_weight, jnp.zeros_like(route_weight)), axis=1))
        chosen = jnp.nonzero(jnp.any(match_mask, axis=1), size=most_rows, fill_value=row_count)[0].astype(jnp.int32)
        slot_rows = padded[chosen]
        hidden = (jax.nn.silu(jnp.dot(slot_rows, gate_half, preferred_element_type=jnp.float32)) * jnp.dot(slot_rows, up_half, preferred_element_type=jnp.float32)).astype(jnp.bfloat16)
        part_out = jnp.dot(hidden, down_half, preferred_element_type=jnp.float32).astype(jnp.bfloat16).astype(jnp.float32)
        weight_pad = jnp.concatenate([weight_sum, jnp.zeros((1,), weight_sum.dtype)])[chosen]
        running = running.at[chosen].add(weight_pad[:, None] * part_out, mode='drop')
        return (running, None)
    halves = jnp.arange(expert_gate.shape[0], dtype=jnp.int32)
    running, _ = lax.scan(one_half, jnp.zeros((row_count, D), jnp.float32), (halves, expert_gate, expert_up, expert_down))
    return running

def reference(tokens, cache_latent, cache_rope, cache_lengths, expert_ids, route_weight, attn_gain, q_gain, kv_gain, moe_gain, w_qdown, w_kvdown, w_krope, w_qup, w_kup, w_vup, w_out, expert_gate, expert_up, expert_down):
    row_count = tokens.shape[0]
    score_scale = (NOPE_DIM + ROPE_DIM) ** (-0.5)
    normed = norm_gain(tokens, attn_gain).astype(jnp.bfloat16)
    q_low = norm_gain(jnp.dot(normed, w_qdown, preferred_element_type=jnp.float32), q_gain).astype(jnp.bfloat16)
    query_all = jnp.dot(q_low, w_qup, preferred_element_type=jnp.float32).reshape(row_count, HEADS, NOPE_DIM + ROPE_DIM)
    angles = rotary_angles(cache_lengths)
    q_nope = query_all[:, :, :NOPE_DIM].astype(jnp.bfloat16)
    q_rope = rotate(query_all[:, :, NOPE_DIM:], angles[:, None, :]).astype(jnp.bfloat16)
    new_latent = norm_gain(jnp.dot(normed, w_kvdown, preferred_element_type=jnp.float32), kv_gain).astype(jnp.bfloat16)
    new_rope_key = rotate(jnp.dot(normed, w_krope, preferred_element_type=jnp.float32), angles).astype(jnp.bfloat16)
    key_up = w_kup.reshape(KV_RANK, HEADS, NOPE_DIM).astype(jnp.float32)
    q_latent = jnp.einsum('thn,chn->thc', q_nope.astype(jnp.float32), key_up).astype(jnp.bfloat16)
    positions = jnp.arange(CACHE, dtype=jnp.int32)

    def one_sequence(inputs):
        q_lat, q_rot, cached, cached_rope, length, latent, rope_key = inputs
        past = (jnp.dot(q_lat, cached.T, preferred_element_type=jnp.float32) + jnp.dot(q_rot, cached_rope.T, preferred_element_type=jnp.float32)) * score_scale
        past = jnp.where(positions[None, :] < length, past, -jnp.inf)
        own_score = (jnp.dot(q_lat, latent, preferred_element_type=jnp.float32) + jnp.dot(q_rot, rope_key, preferred_element_type=jnp.float32)) * score_scale
        scores = jnp.concatenate([past, own_score[:, None]], axis=1)
        peak = lax.optimization_barrier(jnp.max(scores, axis=1, keepdims=True))
        raw_probs = jnp.exp(scores - peak)
        denom = lax.optimization_barrier(jnp.sum(raw_probs, axis=1, keepdims=True))
        probs = raw_probs.astype(jnp.bfloat16)
        summed = jnp.dot(probs[:, :CACHE], cached, preferred_element_type=jnp.float32) + probs[:, CACHE:].astype(jnp.float32) * latent.astype(jnp.float32)[None, :]
        return (summed / denom).astype(jnp.bfloat16)
    o_latent = lax.map(one_sequence, (q_latent, q_rope, cache_latent, cache_rope, cache_lengths, new_latent, new_rope_key))
    value_up = w_vup.reshape(KV_RANK, HEADS, VALUE_DIM).astype(jnp.float32)
    heads_out = jnp.einsum('thc,chv->thv', o_latent.astype(jnp.float32), value_up).astype(jnp.bfloat16)
    heads_out = heads_out.reshape(row_count, HEADS * VALUE_DIM)
    mixed_attn = (tokens.astype(jnp.float32) + jnp.dot(heads_out, w_out, preferred_element_type=jnp.float32)).astype(jnp.bfloat16)
    moe_in = norm_gain(mixed_attn, moe_gain).astype(jnp.bfloat16)
    moe_out = routed(moe_in, expert_ids, route_weight, expert_gate, expert_up, expert_down)
    mixed = mixed_attn.astype(jnp.float32) + moe_out
    return (mixed, new_latent, new_rope_key)
```

```python
import jax
import jax.numpy as jnp
import numpy as np
from jax import lax
from jax.experimental import pallas as pl
from jax.experimental.pallas import tpu as pltpu
from jax.sharding import PartitionSpec as P

HEADS = 8
NOPE_DIM = 128
ROPE_DIM = 64
VALUE_DIM = 128
GROUP_SIZE = 16
TOP_K = 6
SEQ_DEV = 12
LANES = 128
ROWS = 16
SEQ_STEP = 4
SEQ_AHEAD = 8

EPS = 1e-06
THETA = 10000.0
F32 = jnp.float32
BF16 = jnp.bfloat16


def mm(a, b):
    return jnp.dot(a, b, preferred_element_type=F32)


def mm_t(a, b):
    return lax.dot_general(a, b, (((1,), (1,)), ((), ())), preferred_element_type=F32)


def partner(value, axis, bit):
    mask = 2**bit
    pairs = [(source, source ^ mask) for source in range(lax.axis_size(axis))]
    return lax.ppermute(value, axis, pairs)


def norm_gain(values, gain_vec):
    return values * lax.rsqrt(jnp.mean(values * values, axis=-1, keepdims=True) + EPS) * gain_vec


def capacity_of(half_count):
    group_count = half_count // 2 // GROUP_SIZE
    group_most = min(SEQ_DEV, max(3, 2 * ((SEQ_DEV + group_count - 1) // group_count)))
    return (TOP_K * group_most + GROUP_SIZE - 1) // GROUP_SIZE


def inverse_row():
    half_width = ROPE_DIM // 2
    inverse = THETA ** (-np.arange(half_width) / half_width)
    return np.tile(inverse, LANES // half_width).reshape(1, LANES).astype(np.float32)


def mixer(n_seq, n_pos, width, lat, expert_count, slot_count):
    scale = (NOPE_DIM + ROPE_DIM) ** (-0.5)
    half = width // 2
    chunks = half // LANES

    def body(
        len_hbm,
        tokens_hbm,
        inverse_hbm,
        ids_hbm,
        weight_hbm,
        attn_gain_hbm,
        q_gain_hbm,
        kv_gain_hbm,
        moe_gain_hbm,
        qdown_hbm,
        kvdown_hbm,
        krope_hbm,
        qup_hbm,
        kup_hbm,
        vup_hbm,
        out_hbm,
        latent_hbm,
        rope_hbm,
        gate_hbm,
        up_hbm,
        down_hbm,
        mixed_hbm,
        new_latent_ref,
        new_rope_ref,
        send_ref,
        combine_hbm,
        gate_ref,
        up_ref,
        down_ref,
        len_ref,
        tokens_ref,
        inverse_ref,
        ids_ref,
        weight_ref,
        attn_gain_ref,
        q_gain_ref,
        kv_gain_ref,
        moe_gain_ref,
        mixed_ref,
        combine_ref,
        qdown,
        kvdown,
        krope,
        qup,
        kup,
        vup,
        w_out,
        latent,
        rope,
        q_lat_s,
        q_rope_s,
        o_lat_s,
        rows_s,
        latent_row_s,
        key_row_s,
        w_sem,
        c_sem,
        r_sem,
        s_sem,
        o_sem,
    ):
        small = [
            pltpu.make_async_copy(source, target, s_sem.at[i])
            for i, (source, target) in enumerate(
                (
                    (tokens_hbm, tokens_ref),
                    (attn_gain_hbm, attn_gain_ref),
                    (len_hbm, len_ref),
                    (inverse_hbm, inverse_ref),
                    (ids_hbm, ids_ref),
                    (weight_hbm, weight_ref),
                    (q_gain_hbm, q_gain_ref),
                    (kv_gain_hbm, kv_gain_ref),
                    (moe_gain_hbm, moe_gain_ref),
                )
            )
        ]
        for copy in small:
            copy.start()

        def weight_copy(i):
            pairs = [
                (qdown_hbm, qdown),
                (kvdown_hbm, kvdown),
                (krope_hbm, krope),
                (qup_hbm, qup),
                (kup_hbm, kup),
                (vup_hbm, vup),
                (out_hbm, w_out),
                (gate_hbm, gate_ref),
                (up_hbm, up_ref),
                (down_hbm, down_ref),
            ]
            return pltpu.make_async_copy(pairs[i][0], pairs[i][1], w_sem.at[i])

        def latent_copy(t):
            return pltpu.make_async_copy(latent_hbm.at[t], latent.at[t], c_sem.at[t])

        def rope_copy(t):
            return pltpu.make_async_copy(rope_hbm.at[t], rope.at[t], r_sem.at[t])

        def cache_start(t):
            latent_copy(t).start()
            rope_copy(t).start()

        weight_copy(0).start()
        weight_copy(1).start()

        expert_row = lax.broadcasted_iota(jnp.int32, (expert_count, LANES), 0)
        for copy in small:
            copy.wait()
        token_lane = lax.broadcasted_iota(jnp.int32, (n_seq, LANES), 1)
        token_row = lax.broadcasted_iota(jnp.int32, (n_seq, LANES), 0)
        spread = (token_lane % ROWS == token_row).astype(BF16)
        valid = lax.broadcasted_iota(jnp.int32, (TOP_K, LANES), 1) % ROWS < n_seq
        ids = jnp.where(valid, mm(ids_ref[...].astype(F32).astype(BF16), spread), -1.0)
        ids = ids.astype(jnp.int32)
        weight = weight_ref[...]
        weight_high = weight.astype(BF16)
        weight_low = mm((weight - weight_high.astype(F32)).astype(BF16), spread)
        weight_high = mm(weight_high, spread)
        taken = jnp.zeros((expert_count, LANES), F32)
        share_high = jnp.zeros((expert_count, LANES), F32)
        share_low = jnp.zeros((expert_count, LANES), F32)
        for k in range(TOP_K):
            hit = ids[k : k + 1, :] == expert_row
            taken = jnp.where(hit, 1.0, taken)
            share_high = jnp.where(hit, weight_high[k : k + 1, :], share_high)
            share_low = jnp.where(hit, weight_low[k : k + 1, :], share_low)
        for i in range(2, 5):
            weight_copy(i).start()
        row_a = lax.broadcasted_iota(jnp.int32, (LANES, LANES), 0)
        row_b = lax.broadcasted_iota(jnp.int32, (LANES, LANES), 1)
        before = ((row_a // ROWS == row_b // ROWS) & (row_a < row_b)).astype(BF16)
        rank = mm(taken.astype(BF16), before)
        rank = jnp.where(taken > 0.5, rank, -1.0)
        rows_per = slot_count * chunks
        shape3 = (expert_count, rows_per, LANES)
        sub = lax.broadcasted_iota(jnp.int32, shape3, 1)
        lane3 = lax.broadcasted_iota(jnp.int32, shape3, 2)
        placed = (rank[:, None, :] == (sub // chunks).astype(F32)) & (sub % chunks == lane3 // ROWS)
        flat = (expert_count * rows_per, LANES)
        picked = jnp.where(placed, 1.0, 0.0).reshape(flat).astype(BF16)
        for part, share in ((0, share_high), (1, share_low)):
            back = jnp.where(placed, jnp.broadcast_to(share[:, None, :], shape3), 0.0)
            combine_ref[part] = back.reshape(flat).T.astype(BF16)
        combine_copy = pltpu.make_async_copy(combine_ref, combine_hbm, o_sem.at[0])
        combine_copy.start()
        rows_s[...] = jnp.zeros_like(rows_s)

        tokens = tokens_ref[...].astype(F32)
        normed = norm_gain(tokens, attn_gain_ref[...]).astype(BF16)
        weight_copy(0).wait()
        cache_start(0)
        cache_start(1)
        q_low = norm_gain(mm(normed, qdown[...]), q_gain_ref[...]).astype(BF16)
        weight_copy(1).wait()
        cache_start(2)
        cache_start(3)
        new_latent = norm_gain(mm(normed, kvdown[...]), kv_gain_ref[...]).astype(BF16)
        new_latent_ref[...] = new_latent
        latent_row_s[...] = new_latent.astype(F32)
        weight_copy(2).wait()
        key_raw = mm_t(normed, krope[...])
        low_half = lax.broadcasted_iota(jnp.int32, (n_seq, LANES), 1)
        first_quarter = low_half % ROPE_DIM < ROPE_DIM // 2
        low_half = low_half < ROPE_DIM

        length = jnp.zeros((n_seq, LANES), F32)
        for t in range(n_seq):
            length = jnp.where(token_row == t, len_ref[t].astype(F32), length)
        angle = length * inverse_ref[...]
        cosine = jnp.cos(angle)
        sine = jnp.sin(angle)
        sine = jnp.where(first_quarter, -sine, sine)

        def rotate(v):
            swapped = jnp.where(
                first_quarter,
                pltpu.roll(v, LANES - ROPE_DIM // 2, 1),
                pltpu.roll(v, ROPE_DIM // 2, 1),
            )
            return v * cosine + swapped * sine

        new_key = rotate(jnp.concatenate([key_raw, key_raw], axis=1))
        new_key = new_key.astype(BF16)
        new_rope_ref[...] = new_key[:, :ROPE_DIM]
        key_row_s[...] = jnp.where(low_half, new_key.astype(F32), 0.0)

        weight_copy(3).wait()
        for t in range(4, SEQ_AHEAD):
            cache_start(t)
        query = mm(q_low, qup[...])
        weight_copy(4).wait()
        for pair in range(HEADS // 2):
            base = 3 * LANES * pair
            first = query[:, base : base + LANES]
            middle = query[:, base + LANES : base + 2 * LANES]
            last = query[:, base + 2 * LANES : base + 3 * LANES]
            second = jnp.where(
                low_half, pltpu.roll(middle, ROPE_DIM, 1), pltpu.roll(last, ROPE_DIM, 1)
            )
            both = rotate(jnp.where(low_half, middle, last))
            for side, nope in ((0, first), (1, second)):
                head = 2 * pair + side
                q_lat_s[:, head, :] = mm_t(
                    nope.astype(BF16), kup[:, head * NOPE_DIM : (head + 1) * NOPE_DIM]
                )
                turned = both if side == 0 else pltpu.roll(both, ROPE_DIM, 1)
                q_rope_s[:, head, :] = turned

        position = lax.broadcasted_iota(jnp.int32, (HEADS, n_pos), 1)

        def step(group, carry):
            start = group * SEQ_STEP
            for j in range(SEQ_STEP):

                @pl.when(start + j + SEQ_AHEAD < n_seq)
                def _(ahead=start + j + SEQ_AHEAD):
                    cache_start(ahead)

            @pl.when((start + SEQ_AHEAD >= n_seq) & (start + SEQ_AHEAD < n_seq + SEQ_STEP))
            def _():
                for i in range(5, 10):
                    weight_copy(i).start()

            for j in range(SEQ_STEP):
                latent_copy(start + j).wait()
                rope_copy(start + j).wait()
            for j in range(SEQ_STEP):
                t = start + j
                q_lat = q_lat_s[t].astype(BF16)
                q_rope = q_rope_s[t].astype(BF16)
                own_row = latent_row_s[pl.ds(t, 1), :]
                own_key = key_row_s[pl.ds(t, 1), :]
                own = (
                    jnp.sum(q_lat.astype(F32) * own_row, axis=1, keepdims=True)
                    + jnp.sum(q_rope.astype(F32) * own_key, axis=1, keepdims=True)
                ) * scale
                scores = (
                    mm_t(q_lat, latent[t]) + mm(q_rope[:, :ROPE_DIM], rope[t])
                ) * scale
                scores = jnp.where(position < len_ref[t], scores, -jnp.inf)
                peak = jnp.maximum(jnp.max(scores, axis=1, keepdims=True), own)
                probs = jnp.exp(scores - peak)
                own_prob = jnp.exp(own - peak)
                total = jnp.sum(probs, axis=1, keepdims=True) + own_prob
                summed = mm(probs.astype(BF16), latent[t]) + own_prob.astype(BF16).astype(F32) * own_row
                o_lat_s[:, pl.ds(t, 1), :] = (summed / total)[:, None, :]
            return carry

        lax.fori_loop(0, n_seq // SEQ_STEP, step, 0)

        weight_copy(5).wait()
        parts = []
        for head in range(HEADS):
            parts.append(
                mm(
                    o_lat_s[head].astype(BF16),
                    vup[:, head * VALUE_DIM : (head + 1) * VALUE_DIM],
                ).astype(BF16)
            )
        heads_out = jnp.concatenate(parts, axis=1)
        weight_copy(6).wait()
        for i in range(7, 10):
            weight_copy(i).wait()
        mixed = (tokens + mm(heads_out, w_out[...])).astype(BF16).astype(F32)
        mixed_ref[...] = mixed
        mixed_copy = pltpu.make_async_copy(mixed_ref, mixed_hbm, o_sem.at[1])
        mixed_copy.start()
        moe_in = norm_gain(mixed, moe_gain_ref[...])
        for side in range(2):
            for r in range(chunks):
                col = side * half + r * LANES
                rows_s[side, r * ROWS : r * ROWS + n_seq, :] = moe_in[:, col : col + LANES]
            out = mm(picked, rows_s[side].astype(BF16)).astype(BF16)
            send_ref[:, side] = out.reshape(shape3)
        combine_copy.wait()
        mixed_copy.wait()

    return body


def run_mixer(tokens, cache_latent, cache_rope, cache_lengths, ids, weights, gains, mats, experts, half_count):
    n_seq, width = tokens.shape
    _, n_pos, lat = cache_latent.shape
    expert_count = half_count // 2
    slot_count = capacity_of(half_count)
    chunks = width // 2 // LANES
    rows_per = slot_count * chunks
    vmem = pl.BlockSpec(memory_space=pltpu.VMEM)
    hbm = pl.BlockSpec(memory_space=pltpu.HBM)
    small = [
        cache_lengths,
        tokens,
        jnp.asarray(inverse_row()),
        ids.T,
        weights.T,
        *[g.reshape(1, -1) for g in gains],
    ]
    return pl.pallas_call(
        mixer(n_seq, n_pos, width, lat, expert_count, slot_count),
        out_shape=(
            pltpu.HBM((n_seq, width), F32),
            jax.ShapeDtypeStruct((n_seq, lat), BF16),
            jax.ShapeDtypeStruct((n_seq, ROPE_DIM), BF16),
            jax.ShapeDtypeStruct((expert_count, 2, rows_per, LANES), BF16),
            pltpu.HBM((2, LANES, expert_count * rows_per), BF16),
            *[jax.ShapeDtypeStruct(m.shape, BF16) for m in experts],
        ),
        in_specs=[hbm] * (len(small) + len(mats) + 2 + len(experts)),
        out_specs=(hbm, vmem, vmem, vmem, hbm) + (vmem,) * len(experts),
        scratch_shapes=[pltpu.SMEM((n_seq,), jnp.int32)]
        + [pltpu.VMEM(m.shape, m.dtype) for m in small[1:]]
        + [
            pltpu.VMEM((n_seq, width), F32),
            pltpu.VMEM((2, LANES, expert_count * rows_per), BF16),
        ]
        + [pltpu.VMEM(m.shape, BF16) for m in mats]
        + [
            pltpu.VMEM((n_seq, n_pos, lat), BF16),
            pltpu.VMEM((n_seq, ROPE_DIM, n_pos), BF16),
            pltpu.VMEM((n_seq, HEADS, lat), F32),
            pltpu.VMEM((n_seq, HEADS, LANES), F32),
            pltpu.VMEM((HEADS, n_seq, lat), F32),
            pltpu.VMEM((2, chunks * ROWS, LANES), F32),
            pltpu.VMEM((n_seq, lat), F32),
            pltpu.VMEM((n_seq, LANES), F32),
            pltpu.SemaphoreType.DMA((len(mats) + len(experts),)),
            pltpu.SemaphoreType.DMA((n_seq,)),
            pltpu.SemaphoreType.DMA((n_seq,)),
            pltpu.SemaphoreType.DMA((len(small),)),
            pltpu.SemaphoreType.DMA((2,)),
        ],
        compiler_params=pltpu.CompilerParams(vmem_limit_bytes=44 * 1024 * 1024),
        name="mixer",
    )(
        *[
            pltpu.with_memory_space_constraint(m, pltpu.HBM)
            for m in (*small, *mats, cache_latent, jnp.swapaxes(cache_rope, 1, 2), *experts)
        ],
    )


def expert_kernel(rows, chunks):
    half = chunks * LANES

    def body(side_ref, own_ref, other_ref, gate_ref, up_ref, down_ref, keep_ref, pass_ref, wide):
        side = side_ref[0]
        halves = []
        for slot, ref in ((0, own_ref), (1, other_ref)):
            wide[slot] = ref[...].astype(F32)
            cols = [wide[slot, pl.ds(r, rows, stride=chunks), :].astype(BF16) for r in range(chunks)]
            halves.append(jnp.concatenate(cols, axis=1))
        here = pl.ds(pl.multiple_of(side * half, half), half)
        there = pl.ds(pl.multiple_of((1 - side) * half, half), half)
        gate = mm(halves[0], gate_ref[here, :]) + mm(halves[1], gate_ref[there, :])
        up = mm(halves[0], up_ref[here, :]) + mm(halves[1], up_ref[there, :])
        hidden = (gate * jax.nn.sigmoid(gate) * up).astype(BF16)
        for slot, cols, ref in ((0, there, pass_ref), (1, here, keep_ref)):
            out = mm(hidden, down_ref[:, cols])
            for r in range(chunks):
                wide[slot, pl.ds(r, rows, stride=chunks), :] = out[:, r * LANES : (r + 1) * LANES]
            ref[...] = wide[slot].astype(BF16)

    return body


def run_expert(side, own, other, gate, up, down):
    count, _ = own.shape
    chunks = gate.shape[0] // 2 // LANES
    vmem = pl.BlockSpec(memory_space=pltpu.VMEM)
    return pl.pallas_call(
        expert_kernel(count // chunks, chunks),
        out_shape=(jax.ShapeDtypeStruct(own.shape, BF16),) * 2,
        in_specs=[pl.BlockSpec(memory_space=pltpu.SMEM)] + [vmem] * 5,
        out_specs=(vmem, vmem),
        scratch_shapes=[pltpu.VMEM((2, count, LANES), F32)],
        compiler_params=pltpu.CompilerParams(vmem_limit_bytes=40 * 1024 * 1024),
        name="expert_half",
    )(side, own, other, gate, up, down)


def combine_kernel(n_seq, chunks):
    half = chunks * LANES

    def body(mixed_ref, combine_ref, rows_ref, out_ref):
        expert_count, _, rows_per, _ = rows_ref.shape
        for side in range(2):
            rows = rows_ref[:, side].reshape(expert_count * rows_per, LANES)
            total = mm(combine_ref[0], rows) + mm(combine_ref[1], rows)
            for r in range(chunks):
                col = slice(side * half + r * LANES, side * half + (r + 1) * LANES)
                out_ref[:, col] = mixed_ref[:, col] + total[r * ROWS : r * ROWS + n_seq, :]

    return body


def run_combine(mixed, combine, rows):
    n_seq, width = mixed.shape
    vmem = pl.BlockSpec(memory_space=pltpu.VMEM)
    return pl.pallas_call(
        combine_kernel(n_seq, width // 2 // LANES),
        out_shape=jax.ShapeDtypeStruct(mixed.shape, F32),
        in_specs=[vmem] * 3,
        out_specs=vmem,
        compiler_params=pltpu.CompilerParams(vmem_limit_bytes=40 * 1024 * 1024),
        name="combine",
    )(mixed, combine, rows)


def shards(
    tokens,
    cache_latent,
    cache_rope,
    cache_lengths,
    expert_ids,
    route_weight,
    attn_gain,
    q_gain,
    kv_gain,
    moe_gain,
    w_qdown,
    w_kvdown,
    w_krope,
    w_qup,
    w_kup,
    w_vup,
    w_out,
    expert_gate,
    expert_up,
    expert_down,
):
    half_count = lax.axis_size("ep")
    mixed_attn, new_latent, new_rope_key, send, combine, *experts = run_mixer(
        tokens,
        cache_latent,
        cache_rope,
        cache_lengths,
        expert_ids,
        route_weight,
        (attn_gain, q_gain, kv_gain, moe_gain),
        (w_qdown, w_kvdown, w_krope.T, w_qup, w_kup, w_vup, w_out),
        (expert_gate[0], expert_up[0], expert_down[0]),
        half_count,
    )
    block = send.shape[2]
    send = send.reshape(half_count, block, LANES)
    own = lax.all_to_all(send, "ep", split_axis=0, concat_axis=0, tiled=True)
    other = partner(own, "ep", 0)
    side = (lax.axis_index("ep") % 2).reshape(1).astype(jnp.int32)
    flat = (half_count * block, LANES)
    keep, give = run_expert(
        side, own.reshape(flat), other.reshape(flat), *experts
    )
    given = partner(give, "ep", 0)
    pair_sum = (keep.astype(F32) + given.astype(F32)).astype(BF16)
    returned = lax.all_to_all(
        pair_sum.reshape(half_count, block, LANES), "ep", split_axis=0, concat_axis=0, tiled=True
    )
    mixed = run_combine(mixed_attn, combine, returned.reshape(half_count // 2, 2, block, LANES))
    return (mixed, new_latent, new_rope_key)


def solution(mesh):
    placed = (
        P("ep", None),
        P("ep", None, None),
        P("ep", None, None),
        P("ep"),
        P("ep", None),
        P("ep", None),
        P(),
        P(),
        P(),
        P(),
        P(),
        P(),
        P(),
        P(),
        P(),
        P(),
        P(),
        P("ep", None, None),
        P("ep", None, None),
        P("ep", None, None),
    )
    return jax.shard_map(
        shards,
        mesh=mesh,
        in_specs=placed,
        out_specs=(P("ep", None), P("ep", None), P("ep", None)),
        check_vma=False,
    )
```

```python
import jax
import jax.numpy as jnp
import numpy as np
from jax import lax
from jax.experimental import pallas as pl
from jax.experimental.pallas import tpu as pltpu
from jax.sharding import PartitionSpec as P

HEADS = 8
NOPE_DIM = 128
ROPE_DIM = 64
VALUE_DIM = 128
GROUP_SIZE = 16
TOP_K = 6
SEQ_DEV = 12
LANES = 128
ROWS = 16
SEQ_STEP = 4
GROUPS_AHEAD = 3
BLOCK_POS = 256

EPS = 1e-06
THETA = 10000.0
F32 = jnp.float32
BF16 = jnp.bfloat16


def mm(a, b):
    return jnp.dot(a, b, preferred_element_type=F32)


def mm_t(a, b):
    return lax.dot_general(a, b, (((1,), (1,)), ((), ())), preferred_element_type=F32)


def partner(value, axis, bit):
    mask = 2**bit
    pairs = [(source, source ^ mask) for source in range(lax.axis_size(axis))]
    return lax.ppermute(value, axis, pairs)


def norm_gain(values, gain_vec):
    return values * lax.rsqrt(jnp.mean(values * values, axis=-1, keepdims=True) + EPS) * gain_vec


def capacity_of(half_count):
    group_count = half_count // 2 // GROUP_SIZE
    group_most = min(SEQ_DEV, max(3, 2 * ((SEQ_DEV + group_count - 1) // group_count)))
    return (TOP_K * group_most + GROUP_SIZE - 1) // GROUP_SIZE


def inverse_row():
    half_width = ROPE_DIM // 2
    inverse = THETA ** (-np.arange(half_width) / half_width)
    return np.tile(inverse, LANES // half_width).reshape(1, LANES).astype(np.float32)


def mixer(n_seq, n_pos, width, lat, expert_count, slot_count):
    scale = (NOPE_DIM + ROPE_DIM) ** (-0.5)
    half = width // 2
    chunks = half // LANES

    def body(
        len_hbm,
        tokens_hbm,
        inverse_hbm,
        ids_hbm,
        weight_hbm,
        attn_gain_hbm,
        q_gain_hbm,
        kv_gain_hbm,
        moe_gain_hbm,
        qdown_hbm,
        kvdown_hbm,
        krope_hbm,
        qup_hbm,
        kup_hbm,
        vup_hbm,
        out_hbm,
        latent_hbm,
        rope_hbm,
        gate_hbm,
        up_hbm,
        down_hbm,
        mixed_hbm,
        new_latent_ref,
        new_rope_ref,
        send_ref,
        combine_hbm,
        gate_ref,
        up_ref,
        down_ref,
        len_ref,
        tokens_ref,
        inverse_ref,
        ids_ref,
        weight_ref,
        attn_gain_ref,
        q_gain_ref,
        kv_gain_ref,
        moe_gain_ref,
        mixed_ref,
        combine_ref,
        qdown,
        kvdown,
        krope,
        qup,
        kup,
        vup,
        w_out,
        latent,
        rope,
        order_s,
        blocks_s,
        score_s,
        prob_s,
        sum_s,
        q_lat_s,
        q_rope_s,
        o_lat_s,
        rows_s,
        latent_row_s,
        key_row_s,
        w_sem,
        c_sem,
        r_sem,
        s_sem,
        o_sem,
    ):
        small = [
            pltpu.make_async_copy(source, target, s_sem.at[i])
            for i, (source, target) in enumerate(
                (
                    (tokens_hbm, tokens_ref),
                    (attn_gain_hbm, attn_gain_ref),
                    (len_hbm, len_ref),
                    (inverse_hbm, inverse_ref),
                    (ids_hbm, ids_ref),
                    (weight_hbm, weight_ref),
                    (q_gain_hbm, q_gain_ref),
                    (kv_gain_hbm, kv_gain_ref),
                    (moe_gain_hbm, moe_gain_ref),
                )
            )
        ]
        for copy in small:
            copy.start()

        def weight_copy(i):
            pairs = [
                (qdown_hbm, qdown),
                (kvdown_hbm, kvdown),
                (krope_hbm, krope),
                (qup_hbm, qup),
                (kup_hbm, kup),
                (vup_hbm, vup),
                (out_hbm, w_out),
                (gate_hbm, gate_ref),
                (up_hbm, up_ref),
                (down_hbm, down_ref),
            ]
            return pltpu.make_async_copy(pairs[i][0], pairs[i][1], w_sem.at[i])

        group_count = n_seq // SEQ_STEP
        most_blocks = pl.cdiv(n_pos, BLOCK_POS)

        def latent_copy(group, j, block):
            slot = group * SEQ_STEP + j
            rows = pl.ds(block * BLOCK_POS, min(BLOCK_POS, n_pos - block * BLOCK_POS))
            return pltpu.make_async_copy(
                latent_hbm.at[order_s[slot], rows, :],
                latent.at[slot, rows, :],
                c_sem.at[slot, block],
            )

        def rope_copy(group, j):
            slot = group * SEQ_STEP + j
            return pltpu.make_async_copy(rope_hbm.at[order_s[slot]], rope.at[slot], r_sem.at[slot])

        def each_copy(group, act):
            for block in range(most_blocks):

                @pl.when(blocks_s[group] > block)
                def _(block=block):
                    for j in range(SEQ_STEP):
                        act(latent_copy(group, j, block))

            for j in range(SEQ_STEP):
                act(rope_copy(group, j))

        def cache_start(group):
            each_copy(group, lambda copy: copy.start())

        weight_copy(0).start()
        weight_copy(1).start()

        small[2].wait()
        lengths = [len_ref[t] for t in range(n_seq)]
        places = [jnp.int32(0)] * n_seq
        for i in range(n_seq):
            for j in range(i):
                later = (lengths[i] > lengths[j]).astype(jnp.int32)
                places[j] = places[j] + later
                places[i] = places[i] + (1 - later)
        for t in range(n_seq):
            order_s[places[t]] = jnp.int32(t)
        for group in range(group_count):
            longest = len_ref[order_s[group * SEQ_STEP]]
            blocks_s[group] = (longest + (BLOCK_POS - 1)) // BLOCK_POS

        expert_row = lax.broadcasted_iota(jnp.int32, (expert_count, LANES), 0)
        for i, copy in enumerate(small):
            if i != 2:
                copy.wait()
        token_lane = lax.broadcasted_iota(jnp.int32, (n_seq, LANES), 1)
        token_row = lax.broadcasted_iota(jnp.int32, (n_seq, LANES), 0)
        spread = (token_lane % ROWS == token_row).astype(BF16)
        valid = lax.broadcasted_iota(jnp.int32, (TOP_K, LANES), 1) % ROWS < n_seq
        ids = jnp.where(valid, mm(ids_ref[...].astype(F32).astype(BF16), spread), -1.0)
        ids = ids.astype(jnp.int32)
        weight = weight_ref[...]
        weight_high = weight.astype(BF16)
        weight_low = mm((weight - weight_high.astype(F32)).astype(BF16), spread)
        weight_high = mm(weight_high, spread)
        taken = jnp.zeros((expert_count, LANES), F32)
        share_high = jnp.zeros((expert_count, LANES), F32)
        share_low = jnp.zeros((expert_count, LANES), F32)
        for k in range(TOP_K):
            hit = ids[k : k + 1, :] == expert_row
            taken = jnp.where(hit, 1.0, taken)
            share_high = jnp.where(hit, weight_high[k : k + 1, :], share_high)
            share_low = jnp.where(hit, weight_low[k : k + 1, :], share_low)
        for i in range(2, 5):
            weight_copy(i).start()
        row_a = lax.broadcasted_iota(jnp.int32, (LANES, LANES), 0)
        row_b = lax.broadcasted_iota(jnp.int32, (LANES, LANES), 1)
        before = ((row_a // ROWS == row_b // ROWS) & (row_a < row_b)).astype(BF16)
        rank = mm(taken.astype(BF16), before)
        rank = jnp.where(taken > 0.5, rank, -1.0)
        rows_per = slot_count * chunks
        shape3 = (expert_count, rows_per, LANES)
        sub = lax.broadcasted_iota(jnp.int32, shape3, 1)
        lane3 = lax.broadcasted_iota(jnp.int32, shape3, 2)
        placed = (rank[:, None, :] == (sub // chunks).astype(F32)) & (sub % chunks == lane3 // ROWS)
        flat = (expert_count * rows_per, LANES)
        picked = jnp.where(placed, 1.0, 0.0).reshape(flat).astype(BF16)
        for part, share in ((0, share_high), (1, share_low)):
            back = jnp.where(placed, jnp.broadcast_to(share[:, None, :], shape3), 0.0)
            combine_ref[part] = back.reshape(flat).T.astype(BF16)
        combine_copy = pltpu.make_async_copy(combine_ref, combine_hbm, o_sem.at[0])
        combine_copy.start()
        rows_s[...] = jnp.zeros_like(rows_s)

        tokens = tokens_ref[...].astype(F32)
        normed = norm_gain(tokens, attn_gain_ref[...]).astype(BF16)
        weight_copy(0).wait()
        cache_start(0)
        q_low = norm_gain(mm(normed, qdown[...]), q_gain_ref[...]).astype(BF16)
        weight_copy(1).wait()
        cache_start(1)
        new_latent = norm_gain(mm(normed, kvdown[...]), kv_gain_ref[...]).astype(BF16)
        new_latent_ref[...] = new_latent
        latent_row_s[...] = new_latent.astype(F32)
        weight_copy(2).wait()
        key_raw = mm_t(normed, krope[...])
        low_half = lax.broadcasted_iota(jnp.int32, (n_seq, LANES), 1)
        first_quarter = low_half % ROPE_DIM < ROPE_DIM // 2
        low_half = low_half < ROPE_DIM

        length = jnp.zeros((n_seq, LANES), F32)
        for t in range(n_seq):
            length = jnp.where(token_row == t, len_ref[t].astype(F32), length)
        angle = length * inverse_ref[...]
        cosine = jnp.cos(angle)
        sine = jnp.sin(angle)
        sine = jnp.where(first_quarter, -sine, sine)

        def rotate(v):
            swapped = jnp.where(
                first_quarter,
                pltpu.roll(v, LANES - ROPE_DIM // 2, 1),
                pltpu.roll(v, ROPE_DIM // 2, 1),
            )
            return v * cosine + swapped * sine

        new_key = rotate(jnp.concatenate([key_raw, key_raw], axis=1))
        new_key = new_key.astype(BF16)
        new_rope_ref[...] = new_key[:, :ROPE_DIM]
        key_row_s[...] = jnp.where(low_half, new_key.astype(F32), 0.0)

        weight_copy(3).wait()
        for group in range(2, GROUPS_AHEAD):
            cache_start(group)
        query = mm(q_low, qup[...])
        weight_copy(4).wait()
        for pair in range(HEADS // 2):
            base = 3 * LANES * pair
            first = query[:, base : base + LANES]
            middle = query[:, base + LANES : base + 2 * LANES]
            last = query[:, base + 2 * LANES : base + 3 * LANES]
            second = jnp.where(
                low_half, pltpu.roll(middle, ROPE_DIM, 1), pltpu.roll(last, ROPE_DIM, 1)
            )
            both = rotate(jnp.where(low_half, middle, last))
            for side, nope in ((0, first), (1, second)):
                head = 2 * pair + side
                q_lat_s[:, head, :] = mm_t(
                    nope.astype(BF16), kup[:, head * NOPE_DIM : (head + 1) * NOPE_DIM]
                )
                turned = both if side == 0 else pltpu.roll(both, ROPE_DIM, 1)
                q_rope_s[:, head, :] = turned

        def for_blocks(group, act):
            for block in range(most_blocks):

                @pl.when(blocks_s[group] == block + 1)
                def _(count=min(n_pos, (block + 1) * BLOCK_POS)):
                    act(group, count)

        def score(group, count):
            for j in range(SEQ_STEP):
                slot = group * SEQ_STEP + j
                t = order_s[slot]
                q_lat = q_lat_s[t].astype(BF16)
                q_rope = q_rope_s[t].astype(BF16)
                score_s[slot, :, :count] = mm_t(q_lat, latent[slot, :count, :]) + mm(
                    q_rope[:, :ROPE_DIM], rope[slot, :, :count]
                )

        def weigh(group, count):
            for j in range(SEQ_STEP):
                slot = group * SEQ_STEP + j
                sum_s[slot] = mm(prob_s[slot, :, :count].astype(BF16), latent[slot, :count, :])

        def score_step(group, carry):
            @pl.when(group + GROUPS_AHEAD < group_count)
            def _():
                cache_start(group + GROUPS_AHEAD)

            each_copy(group, lambda copy: copy.wait())

            @pl.when(group == 0)
            def _():
                weight_copy(5).start()
                weight_copy(6).start()

            @pl.when(group == group_count - 1)
            def _():
                for i in range(7, 10):
                    weight_copy(i).start()

            for_blocks(group, score)
            return carry

        def weigh_step(group, carry):
            for_blocks(group, weigh)
            return carry

        lax.fori_loop(0, group_count, score_step, 0)

        position = lax.broadcasted_iota(jnp.int32, (HEADS, n_pos), 1)
        ends = []
        for slot in range(n_seq):
            t = order_s[slot]
            own_row = latent_row_s[pl.ds(t, 1), :]
            own_key = key_row_s[pl.ds(t, 1), :]
            own = (
                jnp.sum(q_lat_s[t].astype(BF16).astype(F32) * own_row, axis=1, keepdims=True)
                + jnp.sum(q_rope_s[t].astype(BF16).astype(F32) * own_key, axis=1, keepdims=True)
            ) * scale
            scores = jnp.where(position < len_ref[t], score_s[slot] * scale, -jnp.inf)
            peak = jnp.maximum(jnp.max(scores, axis=1, keepdims=True), own)
            probs = jnp.exp(scores - peak)
            own_prob = jnp.exp(own - peak)
            ends.append((own_prob, jnp.sum(probs, axis=1, keepdims=True) + own_prob))
            prob_s[slot] = probs

        lax.fori_loop(0, group_count, weigh_step, 0)

        for slot, (own_prob, total) in enumerate(ends):
            t = order_s[slot]
            own_row = latent_row_s[pl.ds(t, 1), :]
            summed = sum_s[slot] + own_prob.astype(BF16).astype(F32) * own_row
            o_lat_s[:, pl.ds(t, 1), :] = (summed / total)[:, None, :]

        weight_copy(5).wait()
        parts = []
        for head in range(HEADS):
            parts.append(
                mm(
                    o_lat_s[head].astype(BF16),
                    vup[:, head * VALUE_DIM : (head + 1) * VALUE_DIM],
                ).astype(BF16)
            )
        heads_out = jnp.concatenate(parts, axis=1)
        weight_copy(6).wait()
        for i in range(7, 10):
            weight_copy(i).wait()
        mixed = (tokens + mm(heads_out, w_out[...])).astype(BF16).astype(F32)
        mixed_ref[...] = mixed
        mixed_copy = pltpu.make_async_copy(mixed_ref, mixed_hbm, o_sem.at[1])
        mixed_copy.start()
        moe_in = norm_gain(mixed, moe_gain_ref[...])
        for side in range(2):
            for r in range(chunks):
                col = side * half + r * LANES
                rows_s[side, r * ROWS : r * ROWS + n_seq, :] = moe_in[:, col : col + LANES]
            out = mm(picked, rows_s[side].astype(BF16)).astype(BF16)
            send_ref[:, side] = out.reshape(shape3)
        combine_copy.wait()
        mixed_copy.wait()

    return body


def run_mixer(tokens, cache_latent, cache_rope, cache_lengths, ids, weights, gains, mats, experts, half_count):
    n_seq, width = tokens.shape
    _, n_pos, lat = cache_latent.shape
    expert_count = half_count // 2
    slot_count = capacity_of(half_count)
    chunks = width // 2 // LANES
    rows_per = slot_count * chunks
    vmem = pl.BlockSpec(memory_space=pltpu.VMEM)
    hbm = pl.BlockSpec(memory_space=pltpu.HBM)
    small = [
        cache_lengths,
        tokens,
        jnp.asarray(inverse_row()),
        ids.T,
        weights.T,
        *[g.reshape(1, -1) for g in gains],
    ]
    return pl.pallas_call(
        mixer(n_seq, n_pos, width, lat, expert_count, slot_count),
        out_shape=(
            pltpu.HBM((n_seq, width), F32),
            jax.ShapeDtypeStruct((n_seq, lat), BF16),
            jax.ShapeDtypeStruct((n_seq, ROPE_DIM), BF16),
            jax.ShapeDtypeStruct((expert_count, 2, rows_per, LANES), BF16),
            pltpu.HBM((2, LANES, expert_count * rows_per), BF16),
            *[jax.ShapeDtypeStruct(m.shape, BF16) for m in experts],
        ),
        in_specs=[hbm] * (len(small) + len(mats) + 2 + len(experts)),
        out_specs=(hbm, vmem, vmem, vmem, hbm) + (vmem,) * len(experts),
        scratch_shapes=[pltpu.SMEM((n_seq,), jnp.int32)]
        + [pltpu.VMEM(m.shape, m.dtype) for m in small[1:]]
        + [
            pltpu.VMEM((n_seq, width), F32),
            pltpu.VMEM((2, LANES, expert_count * rows_per), BF16),
        ]
        + [pltpu.VMEM(m.shape, BF16) for m in mats]
        + [
            pltpu.VMEM((n_seq, n_pos, lat), BF16),
            pltpu.VMEM((n_seq, ROPE_DIM, n_pos), BF16),
            pltpu.SMEM((n_seq,), jnp.int32),
            pltpu.SMEM((n_seq,), jnp.int32),
            pltpu.VMEM((n_seq, HEADS, n_pos), F32),
            pltpu.VMEM((n_seq, HEADS, n_pos), F32),
            pltpu.VMEM((n_seq, HEADS, lat), F32),
            pltpu.VMEM((n_seq, HEADS, lat), F32),
            pltpu.VMEM((n_seq, HEADS, LANES), F32),
            pltpu.VMEM((HEADS, n_seq, lat), F32),
            pltpu.VMEM((2, chunks * ROWS, LANES), F32),
            pltpu.VMEM((n_seq, lat), F32),
            pltpu.VMEM((n_seq, LANES), F32),
            pltpu.SemaphoreType.DMA((len(mats) + len(experts),)),
            pltpu.SemaphoreType.DMA((n_seq, pl.cdiv(n_pos, BLOCK_POS))),
            pltpu.SemaphoreType.DMA((n_seq,)),
            pltpu.SemaphoreType.DMA((len(small),)),
            pltpu.SemaphoreType.DMA((2,)),
        ],
        compiler_params=pltpu.CompilerParams(vmem_limit_bytes=44 * 1024 * 1024),
        name="mixer",
    )(
        *[
            pltpu.with_memory_space_constraint(m, pltpu.HBM)
            for m in (*small, *mats, cache_latent, jnp.swapaxes(cache_rope, 1, 2), *experts)
        ],
    )


def expert_kernel(rows, chunks):
    half = chunks * LANES

    def body(side_ref, own_ref, other_ref, gate_ref, up_ref, down_ref, keep_ref, pass_ref, wide):
        side = side_ref[0]
        halves = []
        for slot, ref in ((0, own_ref), (1, other_ref)):
            wide[slot] = ref[...].astype(F32)
            cols = [wide[slot, pl.ds(r, rows, stride=chunks), :].astype(BF16) for r in range(chunks)]
            halves.append(jnp.concatenate(cols, axis=1))
        here = pl.ds(pl.multiple_of(side * half, half), half)
        there = pl.ds(pl.multiple_of((1 - side) * half, half), half)
        gate = mm(halves[0], gate_ref[here, :]) + mm(halves[1], gate_ref[there, :])
        up = mm(halves[0], up_ref[here, :]) + mm(halves[1], up_ref[there, :])
        hidden = (gate * jax.nn.sigmoid(gate) * up).astype(BF16)
        for slot, cols, ref in ((0, there, pass_ref), (1, here, keep_ref)):
            out = mm(hidden, down_ref[:, cols])
            for r in range(chunks):
                wide[slot, pl.ds(r, rows, stride=chunks), :] = out[:, r * LANES : (r + 1) * LANES]
            ref[...] = wide[slot].astype(BF16)

    return body


def run_expert(side, own, other, gate, up, down):
    count, _ = own.shape
    chunks = gate.shape[0] // 2 // LANES
    vmem = pl.BlockSpec(memory_space=pltpu.VMEM)
    return pl.pallas_call(
        expert_kernel(count // chunks, chunks),
        out_shape=(jax.ShapeDtypeStruct(own.shape, BF16),) * 2,
        in_specs=[pl.BlockSpec(memory_space=pltpu.SMEM)] + [vmem] * 5,
        out_specs=(vmem, vmem),
        scratch_shapes=[pltpu.VMEM((2, count, LANES), F32)],
        compiler_params=pltpu.CompilerParams(vmem_limit_bytes=12 * 1024 * 1024),
        name="expert_half",
    )(side, own, pltpu.with_memory_space_constraint(other, pltpu.VMEM), gate, up, down)


def combine_kernel(n_seq, chunks):
    half = chunks * LANES

    def body(mixed_ref, combine_ref, rows_ref, out_ref):
        expert_count, _, rows_per, _ = rows_ref.shape
        for side in range(2):
            rows = rows_ref[:, side].reshape(expert_count * rows_per, LANES)
            total = mm(combine_ref[0], rows) + mm(combine_ref[1], rows)
            for r in range(chunks):
                col = slice(side * half + r * LANES, side * half + (r + 1) * LANES)
                out_ref[:, col] = mixed_ref[:, col] + total[r * ROWS : r * ROWS + n_seq, :]

    return body


def run_combine(mixed, combine, rows):
    n_seq, width = mixed.shape
    vmem = pl.BlockSpec(memory_space=pltpu.VMEM)
    return pl.pallas_call(
        combine_kernel(n_seq, width // 2 // LANES),
        out_shape=jax.ShapeDtypeStruct(mixed.shape, F32),
        in_specs=[vmem] * 3,
        out_specs=vmem,
        compiler_params=pltpu.CompilerParams(vmem_limit_bytes=12 * 1024 * 1024),
        name="combine",
    )(mixed, combine, rows)


def shards(
    tokens,
    cache_latent,
    cache_rope,
    cache_lengths,
    expert_ids,
    route_weight,
    attn_gain,
    q_gain,
    kv_gain,
    moe_gain,
    w_qdown,
    w_kvdown,
    w_krope,
    w_qup,
    w_kup,
    w_vup,
    w_out,
    expert_gate,
    expert_up,
    expert_down,
):
    half_count = lax.axis_size("ep")
    mixed_attn, new_latent, new_rope_key, send, combine, *experts = run_mixer(
        tokens,
        cache_latent,
        cache_rope,
        cache_lengths,
        expert_ids,
        route_weight,
        (attn_gain, q_gain, kv_gain, moe_gain),
        (w_qdown, w_kvdown, w_krope.T, w_qup, w_kup, w_vup, w_out),
        (expert_gate[0], expert_up[0], expert_down[0]),
        half_count,
    )
    block = send.shape[2]
    send = send.reshape(half_count, block, LANES)
    own = lax.all_to_all(send, "ep", split_axis=0, concat_axis=0, tiled=True)
    own = own.reshape(half_count * block, LANES)
    other = partner(own, "ep", 0)
    side = (lax.axis_index("ep") % 2).reshape(1).astype(jnp.int32)
    keep, give = run_expert(side, own, other, *experts)
    given = partner(give, "ep", 0)
    pair_sum = (keep.astype(F32) + given.astype(F32)).astype(BF16)
    returned = lax.all_to_all(
        pair_sum.reshape(half_count, block, LANES), "ep", split_axis=0, concat_axis=0, tiled=True
    )
    mixed = run_combine(mixed_attn, combine, returned.reshape(half_count // 2, 2, block, LANES))
    return (mixed, new_latent, new_rope_key)


def solution(mesh):
    placed = (
        P("ep", None),
        P("ep", None, None),
        P("ep", None, None),
        P("ep"),
        P("ep", None),
        P("ep", None),
        P(),
        P(),
        P(),
        P(),
        P(),
        P(),
        P(),
        P(),
        P(),
        P(),
        P(),
        P("ep", None, None),
        P("ep", None, None),
        P("ep", None, None),
    )
    return jax.shard_map(
        shards,
        mesh=mesh,
        in_specs=placed,
        out_specs=(P("ep", None), P("ep", None), P("ep", None)),
        check_vma=False,
    )
```

```python
import jax
import jax.numpy as jnp
import numpy as np
from jax import lax
from jax.experimental import pallas as pl
from jax.experimental.pallas import tpu as pltpu
from jax.sharding import PartitionSpec as P

HEADS = 8
NOPE_DIM = 128
ROPE_DIM = 64
VALUE_DIM = 128
GROUP_SIZE = 16
TOP_K = 6
SEQ_DEV = 12
LANES = 128
ROWS = 16
SEQ_STEP = 4
GROUPS_AHEAD = 3
BLOCK_POS = 256

EPS = 1e-06
THETA = 10000.0
F32 = jnp.float32
BF16 = jnp.bfloat16


def mm(a, b):
    return jnp.dot(a, b, preferred_element_type=F32)


def mm_t(a, b):
    return lax.dot_general(a, b, (((1,), (1,)), ((), ())), preferred_element_type=F32)


def partner(value, axis, bit):
    mask = 2**bit
    pairs = [(source, source ^ mask) for source in range(lax.axis_size(axis))]
    return lax.ppermute(value, axis, pairs)


def norm_gain(values, gain_vec):
    return values * lax.rsqrt(jnp.mean(values * values, axis=-1, keepdims=True) + EPS) * gain_vec


def capacity_of(half_count):
    group_count = half_count // 2 // GROUP_SIZE
    group_most = min(SEQ_DEV, max(3, 2 * ((SEQ_DEV + group_count - 1) // group_count)))
    return (TOP_K * group_most + GROUP_SIZE - 1) // GROUP_SIZE


def inverse_row():
    half_width = ROPE_DIM // 2
    inverse = THETA ** (-np.arange(half_width) / half_width)
    return np.tile(inverse, LANES // half_width).reshape(1, LANES).astype(np.float32)


def mixer(n_seq, n_pos, width, lat, expert_count, slot_count):
    scale = (NOPE_DIM + ROPE_DIM) ** (-0.5)
    half = width // 2
    chunks = half // LANES

    def body(
        side_ref,
        len_hbm,
        tokens_hbm,
        inverse_hbm,
        ids_hbm,
        weight_hbm,
        attn_gain_hbm,
        q_gain_hbm,
        kv_gain_hbm,
        moe_gain_hbm,
        qdown_hbm,
        kvdown_hbm,
        krope_hbm,
        qup_hbm,
        kup_hbm,
        vup_hbm,
        out_hbm,
        latent_hbm,
        rope_hbm,
        gate_hbm,
        up_hbm,
        down_hbm,
        mixed_hbm,
        new_latent_ref,
        new_rope_ref,
        send_ref,
        combine_hbm,
        gate_ref,
        up_ref,
        down_ref,
        give_ref,
        len_ref,
        tokens_ref,
        inverse_ref,
        ids_ref,
        weight_ref,
        attn_gain_ref,
        q_gain_ref,
        kv_gain_ref,
        moe_gain_ref,
        mixed_ref,
        combine_ref,
        qdown,
        kvdown,
        krope,
        qup,
        kup,
        vup,
        w_out,
        latent,
        rope,
        order_s,
        blocks_s,
        score_s,
        prob_s,
        sum_s,
        q_lat_s,
        q_rope_s,
        o_lat_s,
        rows_s,
        latent_row_s,
        key_row_s,
        w_sem,
        c_sem,
        r_sem,
        s_sem,
        o_sem,
    ):
        side = side_ref[0]
        hidden = gate_hbm.shape[1]
        here = pl.ds(pl.multiple_of(side * half, half), half)
        there = pl.ds(pl.multiple_of((1 - side) * half, half), half)
        weight_count = 12 + half // hidden
        small = [
            pltpu.make_async_copy(source, target, s_sem.at[i])
            for i, (source, target) in enumerate(
                (
                    (tokens_hbm, tokens_ref),
                    (attn_gain_hbm, attn_gain_ref),
                    (len_hbm, len_ref),
                    (inverse_hbm, inverse_ref),
                    (ids_hbm, ids_ref),
                    (weight_hbm, weight_ref),
                    (q_gain_hbm, q_gain_ref),
                    (kv_gain_hbm, kv_gain_ref),
                    (moe_gain_hbm, moe_gain_ref),
                )
            )
        ]
        for copy in small:
            copy.start()

        def weight_copy(i):
            pairs = [
                (qdown_hbm, qdown),
                (kvdown_hbm, kvdown),
                (krope_hbm, krope),
                (qup_hbm, qup),
                (kup_hbm, kup),
                (vup_hbm, vup),
                (out_hbm, w_out),
                (gate_hbm.at[here, :], gate_ref),
                (up_hbm.at[here, :], up_ref),
                (down_hbm.at[:, here], down_ref),
                (gate_hbm.at[there, :], give_ref.at[:half, :]),
                (up_hbm.at[there, :], give_ref.at[half : 2 * half, :]),
            ]
            for b in range(half // hidden):
                cols = slice(b * hidden, (b + 1) * hidden)
                rows = slice(2 * half + b * hidden, 2 * half + (b + 1) * hidden)
                pairs.append((down_hbm.at[:, there].at[:, cols], give_ref.at[rows, :]))
            return pltpu.make_async_copy(pairs[i][0], pairs[i][1], w_sem.at[i])

        group_count = n_seq // SEQ_STEP
        most_blocks = pl.cdiv(n_pos, BLOCK_POS)

        def latent_copy(group, j, block):
            slot = group * SEQ_STEP + j
            rows = pl.ds(block * BLOCK_POS, min(BLOCK_POS, n_pos - block * BLOCK_POS))
            return pltpu.make_async_copy(
                latent_hbm.at[order_s[slot], rows, :],
                latent.at[slot, rows, :],
                c_sem.at[slot, block],
            )

        def rope_copy(group, j):
            slot = group * SEQ_STEP + j
            return pltpu.make_async_copy(rope_hbm.at[order_s[slot]], rope.at[slot], r_sem.at[slot])

        def each_copy(group, act):
            for block in range(most_blocks):

                @pl.when(blocks_s[group] > block)
                def _(block=block):
                    for j in range(SEQ_STEP):
                        act(latent_copy(group, j, block))

            for j in range(SEQ_STEP):
                act(rope_copy(group, j))

        def cache_start(group):
            each_copy(group, lambda copy: copy.start())

        weight_copy(0).start()
        weight_copy(1).start()

        small[2].wait()
        lengths = [len_ref[t] for t in range(n_seq)]
        places = [jnp.int32(0)] * n_seq
        for i in range(n_seq):
            for j in range(i):
                later = (lengths[i] > lengths[j]).astype(jnp.int32)
                places[j] = places[j] + later
                places[i] = places[i] + (1 - later)
        for t in range(n_seq):
            order_s[places[t]] = jnp.int32(t)
        for group in range(group_count):
            longest = len_ref[order_s[group * SEQ_STEP]]
            blocks_s[group] = (longest + (BLOCK_POS - 1)) // BLOCK_POS

        expert_row = lax.broadcasted_iota(jnp.int32, (expert_count, LANES), 0)
        for i, copy in enumerate(small):
            if i != 2:
                copy.wait()
        token_lane = lax.broadcasted_iota(jnp.int32, (n_seq, LANES), 1)
        token_row = lax.broadcasted_iota(jnp.int32, (n_seq, LANES), 0)
        spread = (token_lane % ROWS == token_row).astype(BF16)
        valid = lax.broadcasted_iota(jnp.int32, (TOP_K, LANES), 1) % ROWS < n_seq
        ids = jnp.where(valid, mm(ids_ref[...].astype(F32).astype(BF16), spread), -1.0)
        ids = ids.astype(jnp.int32)
        weight = weight_ref[...]
        weight_high = weight.astype(BF16)
        weight_low = mm((weight - weight_high.astype(F32)).astype(BF16), spread)
        weight_high = mm(weight_high, spread)
        taken = jnp.zeros((expert_count, LANES), F32)
        share_high = jnp.zeros((expert_count, LANES), F32)
        share_low = jnp.zeros((expert_count, LANES), F32)
        for k in range(TOP_K):
            hit = ids[k : k + 1, :] == expert_row
            taken = jnp.where(hit, 1.0, taken)
            share_high = jnp.where(hit, weight_high[k : k + 1, :], share_high)
            share_low = jnp.where(hit, weight_low[k : k + 1, :], share_low)
        for i in range(2, 5):
            weight_copy(i).start()
        row_a = lax.broadcasted_iota(jnp.int32, (LANES, LANES), 0)
        row_b = lax.broadcasted_iota(jnp.int32, (LANES, LANES), 1)
        before = ((row_a // ROWS == row_b // ROWS) & (row_a < row_b)).astype(BF16)
        rank = mm(taken.astype(BF16), before)
        rank = jnp.where(taken > 0.5, rank, -1.0)
        rows_per = slot_count * chunks
        shape3 = (expert_count, rows_per, LANES)
        sub = lax.broadcasted_iota(jnp.int32, shape3, 1)
        lane3 = lax.broadcasted_iota(jnp.int32, shape3, 2)
        placed = (rank[:, None, :] == (sub // chunks).astype(F32)) & (sub % chunks == lane3 // ROWS)
        flat = (expert_count * rows_per, LANES)
        picked = jnp.where(placed, 1.0, 0.0).reshape(flat).astype(BF16)
        for part, share in ((0, share_high), (1, share_low)):
            back = jnp.where(placed, jnp.broadcast_to(share[:, None, :], shape3), 0.0)
            combine_ref[part] = back.reshape(flat).T.astype(BF16)
        combine_copy = pltpu.make_async_copy(combine_ref, combine_hbm, o_sem.at[0])
        combine_copy.start()
        rows_s[...] = jnp.zeros_like(rows_s)

        tokens = tokens_ref[...].astype(F32)
        normed = norm_gain(tokens, attn_gain_ref[...]).astype(BF16)
        weight_copy(0).wait()
        cache_start(0)
        q_low = norm_gain(mm(normed, qdown[...]), q_gain_ref[...]).astype(BF16)
        weight_copy(1).wait()
        cache_start(1)
        new_latent = norm_gain(mm(normed, kvdown[...]), kv_gain_ref[...]).astype(BF16)
        new_latent_ref[...] = new_latent
        latent_row_s[...] = new_latent.astype(F32)
        weight_copy(2).wait()
        key_raw = mm_t(normed, krope[...])
        low_half = lax.broadcasted_iota(jnp.int32, (n_seq, LANES), 1)
        first_quarter = low_half % ROPE_DIM < ROPE_DIM // 2
        low_half = low_half < ROPE_DIM

        length = jnp.zeros((n_seq, LANES), F32)
        for t in range(n_seq):
            length = jnp.where(token_row == t, len_ref[t].astype(F32), length)
        angle = length * inverse_ref[...]
        cosine = jnp.cos(angle)
        sine = jnp.sin(angle)
        sine = jnp.where(first_quarter, -sine, sine)

        def rotate(v):
            swapped = jnp.where(
                first_quarter,
                pltpu.roll(v, LANES - ROPE_DIM // 2, 1),
                pltpu.roll(v, ROPE_DIM // 2, 1),
            )
            return v * cosine + swapped * sine

        new_key = rotate(jnp.concatenate([key_raw, key_raw], axis=1))
        new_key = new_key.astype(BF16)
        new_rope_ref[...] = new_key[:, :ROPE_DIM]
        key_row_s[...] = jnp.where(low_half, new_key.astype(F32), 0.0)

        weight_copy(3).wait()
        for group in range(2, GROUPS_AHEAD):
            cache_start(group)
        query = mm(q_low, qup[...])
        weight_copy(4).wait()
        for pair in range(HEADS // 2):
            base = 3 * LANES * pair
            first = query[:, base : base + LANES]
            middle = query[:, base + LANES : base + 2 * LANES]
            last = query[:, base + 2 * LANES : base + 3 * LANES]
            second = jnp.where(
                low_half, pltpu.roll(middle, ROPE_DIM, 1), pltpu.roll(last, ROPE_DIM, 1)
            )
            both = rotate(jnp.where(low_half, middle, last))
            for side, nope in ((0, first), (1, second)):
                head = 2 * pair + side
                q_lat_s[:, head, :] = mm_t(
                    nope.astype(BF16), kup[:, head * NOPE_DIM : (head + 1) * NOPE_DIM]
                )
                turned = both if side == 0 else pltpu.roll(both, ROPE_DIM, 1)
                q_rope_s[:, head, :] = turned

        def for_blocks(group, act):
            for block in range(most_blocks):

                @pl.when(blocks_s[group] == block + 1)
                def _(count=min(n_pos, (block + 1) * BLOCK_POS)):
                    act(group, count)

        def score(group, count):
            for j in range(SEQ_STEP):
                slot = group * SEQ_STEP + j
                t = order_s[slot]
                q_lat = q_lat_s[t].astype(BF16)
                q_rope = q_rope_s[t].astype(BF16)
                score_s[slot, :, :count] = mm_t(q_lat, latent[slot, :count, :]) + mm(
                    q_rope[:, :ROPE_DIM], rope[slot, :, :count]
                )

        def weigh(group, count):
            for j in range(SEQ_STEP):
                slot = group * SEQ_STEP + j
                sum_s[slot] = mm(prob_s[slot, :, :count].astype(BF16), latent[slot, :count, :])

        def score_step(group, carry):
            @pl.when(group + GROUPS_AHEAD < group_count)
            def _():
                cache_start(group + GROUPS_AHEAD)

            each_copy(group, lambda copy: copy.wait())

            @pl.when(group == 0)
            def _():
                weight_copy(5).start()
                weight_copy(6).start()

            @pl.when(group == group_count - 1)
            def _():
                for i in range(7, weight_count):
                    weight_copy(i).start()

            for_blocks(group, score)
            return carry

        def weigh_step(group, carry):
            for_blocks(group, weigh)
            return carry

        lax.fori_loop(0, group_count, score_step, 0)

        position = lax.broadcasted_iota(jnp.int32, (HEADS, n_pos), 1)
        ends = []
        for slot in range(n_seq):
            t = order_s[slot]
            own_row = latent_row_s[pl.ds(t, 1), :]
            own_key = key_row_s[pl.ds(t, 1), :]
            own = (
                jnp.sum(q_lat_s[t].astype(BF16).astype(F32) * own_row, axis=1, keepdims=True)
                + jnp.sum(q_rope_s[t].astype(BF16).astype(F32) * own_key, axis=1, keepdims=True)
            ) * scale
            scores = jnp.where(position < len_ref[t], score_s[slot] * scale, -jnp.inf)
            peak = jnp.maximum(jnp.max(scores, axis=1, keepdims=True), own)
            probs = jnp.exp(scores - peak)
            own_prob = jnp.exp(own - peak)
            ends.append((own_prob, jnp.sum(probs, axis=1, keepdims=True) + own_prob))
            prob_s[slot] = probs

        lax.fori_loop(0, group_count, weigh_step, 0)

        for slot, (own_prob, total) in enumerate(ends):
            t = order_s[slot]
            own_row = latent_row_s[pl.ds(t, 1), :]
            summed = sum_s[slot] + own_prob.astype(BF16).astype(F32) * own_row
            o_lat_s[:, pl.ds(t, 1), :] = (summed / total)[:, None, :]

        weight_copy(5).wait()
        parts = []
        for head in range(HEADS):
            parts.append(
                mm(
                    o_lat_s[head].astype(BF16),
                    vup[:, head * VALUE_DIM : (head + 1) * VALUE_DIM],
                ).astype(BF16)
            )
        heads_out = jnp.concatenate(parts, axis=1)
        weight_copy(6).wait()
        for i in range(7, weight_count):
            weight_copy(i).wait()
        mixed = (tokens + mm(heads_out, w_out[...])).astype(BF16).astype(F32)
        mixed_ref[...] = mixed
        mixed_copy = pltpu.make_async_copy(mixed_ref, mixed_hbm, o_sem.at[1])
        mixed_copy.start()
        moe_in = norm_gain(mixed, moe_gain_ref[...])
        for side in range(2):
            for r in range(chunks):
                col = side * half + r * LANES
                rows_s[side, r * ROWS : r * ROWS + n_seq, :] = moe_in[:, col : col + LANES]
            out = mm(picked, rows_s[side].astype(BF16)).astype(BF16)
            send_ref[:, side] = out.reshape(shape3)
        combine_copy.wait()
        mixed_copy.wait()

    return body


def run_mixer(side, tokens, cache_latent, cache_rope, cache_lengths, ids, weights, gains, mats, experts, half_count):
    n_seq, width = tokens.shape
    _, n_pos, lat = cache_latent.shape
    expert_count = half_count // 2
    slot_count = capacity_of(half_count)
    half = width // 2
    hidden = experts[0].shape[1]
    chunks = half // LANES
    rows_per = slot_count * chunks
    vmem = pl.BlockSpec(memory_space=pltpu.VMEM)
    hbm = pl.BlockSpec(memory_space=pltpu.HBM)
    small = [
        cache_lengths,
        tokens,
        jnp.asarray(inverse_row()),
        ids.T,
        weights.T,
        *[g.reshape(1, -1) for g in gains],
    ]
    return pl.pallas_call(
        mixer(n_seq, n_pos, width, lat, expert_count, slot_count),
        out_shape=(
            pltpu.HBM((n_seq, width), F32),
            jax.ShapeDtypeStruct((n_seq, lat), BF16),
            jax.ShapeDtypeStruct((n_seq, ROPE_DIM), BF16),
            jax.ShapeDtypeStruct((expert_count, 2, rows_per, LANES), BF16),
            pltpu.HBM((2, LANES, expert_count * rows_per), BF16),
            jax.ShapeDtypeStruct((half, hidden), BF16),
            jax.ShapeDtypeStruct((half, hidden), BF16),
            jax.ShapeDtypeStruct((hidden, half), BF16),
            jax.ShapeDtypeStruct((3 * half, hidden), BF16),
        ),
        in_specs=[pl.BlockSpec(memory_space=pltpu.SMEM)] + [hbm] * (len(small) + len(mats) + 2 + len(experts)),
        out_specs=(hbm, vmem, vmem, vmem, hbm) + (vmem,) * 4,
        scratch_shapes=[pltpu.SMEM((n_seq,), jnp.int32)]
        + [pltpu.VMEM(m.shape, m.dtype) for m in small[1:]]
        + [
            pltpu.VMEM((n_seq, width), F32),
            pltpu.VMEM((2, LANES, expert_count * rows_per), BF16),
        ]
        + [pltpu.VMEM(m.shape, BF16) for m in mats]
        + [
            pltpu.VMEM((n_seq, n_pos, lat), BF16),
            pltpu.VMEM((n_seq, ROPE_DIM, n_pos), BF16),
            pltpu.SMEM((n_seq,), jnp.int32),
            pltpu.SMEM((n_seq,), jnp.int32),
            pltpu.VMEM((n_seq, HEADS, n_pos), F32),
            pltpu.VMEM((n_seq, HEADS, n_pos), F32),
            pltpu.VMEM((n_seq, HEADS, lat), F32),
            pltpu.VMEM((n_seq, HEADS, lat), F32),
            pltpu.VMEM((n_seq, HEADS, LANES), F32),
            pltpu.VMEM((HEADS, n_seq, lat), F32),
            pltpu.VMEM((2, chunks * ROWS, LANES), F32),
            pltpu.VMEM((n_seq, lat), F32),
            pltpu.VMEM((n_seq, LANES), F32),
            pltpu.SemaphoreType.DMA((12 + half // hidden,)),
            pltpu.SemaphoreType.DMA((n_seq, pl.cdiv(n_pos, BLOCK_POS))),
            pltpu.SemaphoreType.DMA((n_seq,)),
            pltpu.SemaphoreType.DMA((len(small),)),
            pltpu.SemaphoreType.DMA((2,)),
        ],
        compiler_params=pltpu.CompilerParams(vmem_limit_bytes=44 * 1024 * 1024),
        name="mixer",
    )(
        side,
        *[
            pltpu.with_memory_space_constraint(m, pltpu.HBM)
            for m in (*small, *mats, cache_latent, jnp.swapaxes(cache_rope, 1, 2), *experts)
        ],
    )


def inner_kernel(rows, chunks, hidden):
    half = chunks * LANES

    def body(own_ref, gate_ref, up_ref, other_ref, keep_ref, give_ref, wide):
        wide[...] = own_ref[...].astype(F32)
        cols = [wide[pl.ds(r, rows, stride=chunks), :].astype(BF16) for r in range(chunks)]
        own = jnp.concatenate(cols, axis=1)
        mats = (gate_ref[...], up_ref[...], other_ref[:half, :], other_ref[half : 2 * half, :])
        for i, mat in enumerate(mats):
            part = mm(own, mat)
            keep_ref[:, i * hidden : (i + 1) * hidden] = part
            place = (i + 2) % 4
            give_ref[:, place * hidden : (place + 1) * hidden] = part.astype(BF16)

    return body


def run_inner(own, gate, up, other):
    count, _ = own.shape
    half, hidden = gate.shape
    chunks = half // LANES
    rows = count // chunks
    vmem = pl.BlockSpec(memory_space=pltpu.VMEM)
    return pl.pallas_call(
        inner_kernel(rows, chunks, hidden),
        out_shape=(
            jax.ShapeDtypeStruct((rows, 4 * hidden), F32),
            jax.ShapeDtypeStruct((rows, 4 * hidden), BF16),
        ),
        in_specs=[vmem] * 4,
        out_specs=(vmem, vmem),
        scratch_shapes=[pltpu.VMEM((count, LANES), F32)],
        compiler_params=pltpu.CompilerParams(vmem_limit_bytes=12 * 1024 * 1024),
        name="expert_inner",
    )(own, gate, up, other)


def outer_kernel(rows, chunks, hidden):
    half = chunks * LANES

    def body(keep_ref, given_ref, down_ref, other_ref, out_ref, wide):
        total = keep_ref[...] + given_ref[...].astype(F32)
        acts = []
        for start in (0, 2 * hidden):
            gate = total[:, start : start + hidden]
            up = total[:, start + hidden : start + 2 * hidden]
            acts.append((gate * jax.nn.sigmoid(gate) * up).astype(BF16))
        for b in range(half // hidden):
            cols = slice(b * hidden, (b + 1) * hidden)
            base = 2 * half + b * hidden
            out = mm(acts[0], down_ref[:, cols]) + mm(acts[1], other_ref[base : base + hidden, :])
            for r in range(hidden // LANES):
                row = b * (hidden // LANES) + r
                wide[pl.ds(row, rows, stride=chunks), :] = out[:, r * LANES : (r + 1) * LANES]
        out_ref[...] = wide[...].astype(BF16)

    return body


def run_outer(keep, given, down, other):
    rows, _ = keep.shape
    hidden, half = down.shape
    chunks = half // LANES
    vmem = pl.BlockSpec(memory_space=pltpu.VMEM)
    return pl.pallas_call(
        outer_kernel(rows, chunks, hidden),
        out_shape=jax.ShapeDtypeStruct((rows * chunks, LANES), BF16),
        in_specs=[vmem] * 4,
        out_specs=vmem,
        scratch_shapes=[pltpu.VMEM((rows * chunks, LANES), F32)],
        compiler_params=pltpu.CompilerParams(vmem_limit_bytes=12 * 1024 * 1024),
        name="expert_outer",
    )(keep, given, down, other)


def combine_kernel(n_seq, chunks):
    half = chunks * LANES

    def body(mixed_ref, combine_ref, rows_ref, out_ref):
        expert_count, _, rows_per, _ = rows_ref.shape
        for side in range(2):
            rows = rows_ref[:, side].reshape(expert_count * rows_per, LANES)
            total = mm(combine_ref[0], rows) + mm(combine_ref[1], rows)
            for r in range(chunks):
                col = slice(side * half + r * LANES, side * half + (r + 1) * LANES)
                out_ref[:, col] = mixed_ref[:, col] + total[r * ROWS : r * ROWS + n_seq, :]

    return body


def run_combine(mixed, combine, rows):
    n_seq, width = mixed.shape
    vmem = pl.BlockSpec(memory_space=pltpu.VMEM)
    return pl.pallas_call(
        combine_kernel(n_seq, width // 2 // LANES),
        out_shape=jax.ShapeDtypeStruct(mixed.shape, F32),
        in_specs=[vmem] * 3,
        out_specs=vmem,
        compiler_params=pltpu.CompilerParams(vmem_limit_bytes=12 * 1024 * 1024),
        name="combine",
    )(mixed, combine, rows)


def shards(
    tokens,
    cache_latent,
    cache_rope,
    cache_lengths,
    expert_ids,
    route_weight,
    attn_gain,
    q_gain,
    kv_gain,
    moe_gain,
    w_qdown,
    w_kvdown,
    w_krope,
    w_qup,
    w_kup,
    w_vup,
    w_out,
    expert_gate,
    expert_up,
    expert_down,
):
    half_count = lax.axis_size("ep")
    side = jnp.bitwise_and(lax.axis_index("ep"), 1).reshape(1)
    mixed_attn, new_latent, new_rope_key, send, combine, gate, up, down, give = run_mixer(
        side,
        tokens,
        cache_latent,
        cache_rope,
        cache_lengths,
        expert_ids,
        route_weight,
        (attn_gain, q_gain, kv_gain, moe_gain),
        (w_qdown, w_kvdown, w_krope.T, w_qup, w_kup, w_vup, w_out),
        (expert_gate[0], expert_up[0], expert_down[0]),
        half_count,
    )
    block = send.shape[2]
    other = partner(give, "ep", 0)
    own = lax.all_to_all(
        send.reshape(half_count, block, LANES), "ep", split_axis=0, concat_axis=0, tiled=True
    )
    keep, inner = run_inner(own.reshape(half_count * block, LANES), gate, up, other)
    outputs = run_outer(keep, partner(inner, "ep", 0), down, other)
    returned = lax.all_to_all(
        outputs.reshape(half_count, block, LANES), "ep", split_axis=0, concat_axis=0, tiled=True
    )
    mixed = run_combine(mixed_attn, combine, returned.reshape(half_count // 2, 2, block, LANES))
    return (mixed, new_latent, new_rope_key)


def solution(mesh):
    placed = (
        P("ep", None),
        P("ep", None, None),
        P("ep", None, None),
        P("ep"),
        P("ep", None),
        P("ep", None),
        P(),
        P(),
        P(),
        P(),
        P(),
        P(),
        P(),
        P(),
        P(),
        P(),
        P(),
        P("ep", None, None),
        P("ep", None, None),
        P("ep", None, None),
    )
    return jax.shard_map(
        shards,
        mesh=mesh,
        in_specs=placed,
        out_specs=(P("ep", None), P("ep", None), P("ep", None)),
        check_vma=False,
    )
```

```python
import jax
import jax.numpy as jnp
import numpy as np
from jax import lax
from jax.experimental import pallas as pl
from jax.experimental.pallas import tpu as pltpu
from jax.sharding import PartitionSpec as P

HEADS = 8
NOPE_DIM = 128
ROPE_DIM = 64
VALUE_DIM = 128
GROUP_SIZE = 16
TOP_K = 6
SEQ_DEV = 12
LANES = 128
ROWS = 16
SEQ_STEP = 3
GROUPS_AHEAD = 4
BLOCK_POS = 256

EPS = 1e-06
THETA = 10000.0
F32 = jnp.float32
BF16 = jnp.bfloat16


def mm(a, b):
    return jnp.dot(a, b, preferred_element_type=F32)


def mm_t(a, b):
    return lax.dot_general(a, b, (((1,), (1,)), ((), ())), preferred_element_type=F32)


def partner(value, axis, bit):
    mask = 2**bit
    pairs = [(source, source ^ mask) for source in range(lax.axis_size(axis))]
    return lax.ppermute(value, axis, pairs)


def norm_gain(values, gain_vec):
    return values * lax.rsqrt(jnp.mean(values * values, axis=-1, keepdims=True) + EPS) * gain_vec


def capacity_of(half_count):
    group_count = half_count // 2 // GROUP_SIZE
    group_most = min(SEQ_DEV, max(3, 2 * ((SEQ_DEV + group_count - 1) // group_count)))
    return (TOP_K * group_most + GROUP_SIZE - 1) // GROUP_SIZE


def inverse_row():
    half_width = ROPE_DIM // 2
    inverse = THETA ** (-np.arange(half_width) / half_width)
    return np.tile(inverse, LANES // half_width).reshape(1, LANES).astype(np.float32)


def mixer(n_seq, n_pos, width, lat, expert_count, slot_count):
    scale = (NOPE_DIM + ROPE_DIM) ** (-0.5)
    half = width // 2
    chunks = half // LANES

    def body(
        side_ref,
        len_hbm,
        tokens_hbm,
        inverse_hbm,
        ids_hbm,
        weight_hbm,
        attn_gain_hbm,
        q_gain_hbm,
        kv_gain_hbm,
        moe_gain_hbm,
        qdown_hbm,
        kvdown_hbm,
        krope_hbm,
        qup_hbm,
        kup_hbm,
        vup_hbm,
        out_hbm,
        latent_hbm,
        rope_hbm,
        gate_hbm,
        up_hbm,
        down_hbm,
        mixed_hbm,
        new_latent_ref,
        new_rope_ref,
        send_ref,
        combine_hbm,
        gate_ref,
        up_ref,
        down_ref,
        give_ref,
        len_ref,
        tokens_ref,
        inverse_ref,
        ids_ref,
        weight_ref,
        attn_gain_ref,
        q_gain_ref,
        kv_gain_ref,
        moe_gain_ref,
        mixed_ref,
        combine_ref,
        qdown,
        kvdown,
        krope,
        qup,
        kup,
        vup,
        w_out,
        latent,
        rope,
        order_s,
        blocks_s,
        score_s,
        prob_s,
        sum_s,
        q_lat_s,
        q_rope_s,
        o_lat_s,
        rows_s,
        latent_row_s,
        key_row_s,
        w_sem,
        c_sem,
        r_sem,
        s_sem,
        o_sem,
    ):
        side = side_ref[0]
        hidden = gate_hbm.shape[1]
        here = pl.ds(pl.multiple_of(side * half, half), half)
        there = pl.ds(pl.multiple_of((1 - side) * half, half), half)
        weight_count = 12 + half // hidden
        small = [
            pltpu.make_async_copy(source, target, s_sem.at[i])
            for i, (source, target) in enumerate(
                (
                    (tokens_hbm, tokens_ref),
                    (attn_gain_hbm, attn_gain_ref),
                    (len_hbm, len_ref),
                    (inverse_hbm, inverse_ref),
                    (ids_hbm, ids_ref),
                    (weight_hbm, weight_ref),
                    (q_gain_hbm, q_gain_ref),
                    (kv_gain_hbm, kv_gain_ref),
                    (moe_gain_hbm, moe_gain_ref),
                )
            )
        ]
        for copy in small:
            copy.start()

        def weight_copy(i):
            pairs = [
                (qdown_hbm, qdown),
                (kvdown_hbm, kvdown),
                (krope_hbm, krope),
                (qup_hbm, qup),
                (kup_hbm, kup),
                (vup_hbm, vup),
                (out_hbm, w_out),
                (gate_hbm.at[here, :], gate_ref),
                (up_hbm.at[here, :], up_ref),
                (down_hbm.at[:, here], down_ref),
                (gate_hbm.at[there, :], give_ref.at[:half, :]),
                (up_hbm.at[there, :], give_ref.at[half : 2 * half, :]),
            ]
            for b in range(half // hidden):
                cols = slice(b * hidden, (b + 1) * hidden)
                rows = slice(2 * half + b * hidden, 2 * half + (b + 1) * hidden)
                pairs.append((down_hbm.at[:, there].at[:, cols], give_ref.at[rows, :]))
            return pltpu.make_async_copy(pairs[i][0], pairs[i][1], w_sem.at[i])

        group_count = n_seq // SEQ_STEP
        most_blocks = pl.cdiv(n_pos, BLOCK_POS)

        def for_blocks(group, act):
            for block in range(most_blocks):

                @pl.when(blocks_s[group] == block + 1)
                def _(count=min(n_pos, (block + 1) * BLOCK_POS)):
                    act(group, count)

        def latent_copies(group, count):
            slots = [group * SEQ_STEP + j for j in range(SEQ_STEP)]
            return [
                pltpu.make_async_copy(
                    latent_hbm.at[order_s[slot], :count, :],
                    latent.at[slot, :count, :],
                    c_sem.at[slot],
                )
                for slot in slots
            ]

        def start_all(group, count):
            for copy in latent_copies(group, count):
                copy.start()

        def cache_start(group):
            for_blocks(group, start_all)

        rope_copy = pltpu.make_async_copy(rope_hbm, rope, r_sem.at[0])

        weight_copy(0).start()
        weight_copy(1).start()

        small[2].wait()
        lengths = [len_ref[t] for t in range(n_seq)]
        places = [jnp.int32(0)] * n_seq
        for i in range(n_seq):
            for j in range(i):
                later = (lengths[i] > lengths[j]).astype(jnp.int32)
                places[j] = places[j] + later
                places[i] = places[i] + (1 - later)
        for t in range(n_seq):
            order_s[places[t]] = jnp.int32(t)
        for group in range(group_count):
            longest = len_ref[order_s[group * SEQ_STEP]]
            blocks_s[group] = (longest + (BLOCK_POS - 1)) // BLOCK_POS

        expert_row = lax.broadcasted_iota(jnp.int32, (expert_count, LANES), 0)
        for i, copy in enumerate(small):
            if i != 2:
                copy.wait()
        token_lane = lax.broadcasted_iota(jnp.int32, (n_seq, LANES), 1)
        token_row = lax.broadcasted_iota(jnp.int32, (n_seq, LANES), 0)
        spread = (token_lane % ROWS == token_row).astype(BF16)
        valid = lax.broadcasted_iota(jnp.int32, (TOP_K, LANES), 1) % ROWS < n_seq
        ids = jnp.where(valid, mm(ids_ref[...].astype(F32).astype(BF16), spread), -1.0)
        ids = ids.astype(jnp.int32)
        weight = weight_ref[...]
        weight_high = weight.astype(BF16)
        weight_low = mm((weight - weight_high.astype(F32)).astype(BF16), spread)
        weight_high = mm(weight_high, spread)
        taken = jnp.zeros((expert_count, LANES), F32)
        share_high = jnp.zeros((expert_count, LANES), F32)
        share_low = jnp.zeros((expert_count, LANES), F32)
        for k in range(TOP_K):
            hit = ids[k : k + 1, :] == expert_row
            taken = jnp.where(hit, 1.0, taken)
            share_high = jnp.where(hit, weight_high[k : k + 1, :], share_high)
            share_low = jnp.where(hit, weight_low[k : k + 1, :], share_low)
        for i in range(2, 5):
            weight_copy(i).start()
        row_a = lax.broadcasted_iota(jnp.int32, (LANES, LANES), 0)
        row_b = lax.broadcasted_iota(jnp.int32, (LANES, LANES), 1)
        before = ((row_a // ROWS == row_b // ROWS) & (row_a < row_b)).astype(BF16)
        rank = mm(taken.astype(BF16), before)
        rank = jnp.where(taken > 0.5, rank, -1.0)
        rows_per = slot_count * chunks
        shape3 = (expert_count, rows_per, LANES)
        sub = lax.broadcasted_iota(jnp.int32, shape3, 1)
        lane3 = lax.broadcasted_iota(jnp.int32, shape3, 2)
        placed = (rank[:, None, :] == (sub // chunks).astype(F32)) & (sub % chunks == lane3 // ROWS)
        flat = (expert_count * rows_per, LANES)
        picked = jnp.where(placed, 1.0, 0.0).reshape(flat).astype(BF16)
        for part, share in ((0, share_high), (1, share_low)):
            back = jnp.where(placed, jnp.broadcast_to(share[:, None, :], shape3), 0.0)
            combine_ref[part] = back.reshape(flat).T.astype(BF16)
        combine_copy = pltpu.make_async_copy(combine_ref, combine_hbm, o_sem.at[0])
        combine_copy.start()
        rows_s[...] = jnp.zeros_like(rows_s)

        tokens = tokens_ref[...].astype(F32)
        normed = norm_gain(tokens, attn_gain_ref[...]).astype(BF16)
        weight_copy(0).wait()
        rope_copy.start()
        cache_start(0)
        q_low = norm_gain(mm(normed, qdown[...]), q_gain_ref[...]).astype(BF16)
        weight_copy(1).wait()
        cache_start(1)
        new_latent = norm_gain(mm(normed, kvdown[...]), kv_gain_ref[...]).astype(BF16)
        new_latent_ref[...] = new_latent
        latent_row_s[...] = new_latent.astype(F32)
        weight_copy(2).wait()
        key_raw = mm_t(normed, krope[...])
        low_half = lax.broadcasted_iota(jnp.int32, (n_seq, LANES), 1)
        first_quarter = low_half % ROPE_DIM < ROPE_DIM // 2
        low_half = low_half < ROPE_DIM

        length = jnp.zeros((n_seq, LANES), F32)
        for t in range(n_seq):
            length = jnp.where(token_row == t, len_ref[t].astype(F32), length)
        angle = length * inverse_ref[...]
        cosine = jnp.cos(angle)
        sine = jnp.sin(angle)
        sine = jnp.where(first_quarter, -sine, sine)

        def rotate(v):
            swapped = jnp.where(
                first_quarter,
                pltpu.roll(v, LANES - ROPE_DIM // 2, 1),
                pltpu.roll(v, ROPE_DIM // 2, 1),
            )
            return v * cosine + swapped * sine

        new_key = rotate(jnp.concatenate([key_raw, key_raw], axis=1))
        new_key = new_key.astype(BF16)
        new_rope_ref[...] = new_key[:, :ROPE_DIM]
        key_row_s[...] = jnp.where(low_half, new_key.astype(F32), 0.0)

        weight_copy(3).wait()
        for group in range(2, GROUPS_AHEAD):
            cache_start(group)
        query = mm(q_low, qup[...])
        weight_copy(4).wait()
        for pair in range(HEADS // 2):
            base = 3 * LANES * pair
            first = query[:, base : base + LANES]
            middle = query[:, base + LANES : base + 2 * LANES]
            last = query[:, base + 2 * LANES : base + 3 * LANES]
            second = jnp.where(
                low_half, pltpu.roll(middle, ROPE_DIM, 1), pltpu.roll(last, ROPE_DIM, 1)
            )
            both = rotate(jnp.where(low_half, middle, last))
            for side, nope in ((0, first), (1, second)):
                head = 2 * pair + side
                q_lat_s[:, head, :] = mm_t(
                    nope.astype(BF16), kup[:, head * NOPE_DIM : (head + 1) * NOPE_DIM]
                )
                turned = both if side == 0 else pltpu.roll(both, ROPE_DIM, 1)
                q_rope_s[:, head, :] = turned

        def score(group, count):
            for copy in latent_copies(group, count):
                copy.wait()
            for j in range(SEQ_STEP):
                slot = group * SEQ_STEP + j
                t = order_s[slot]
                q_lat = q_lat_s[t].astype(BF16)
                q_rope = q_rope_s[t].astype(BF16)
                score_s[slot, :, :count] = mm_t(q_lat, latent[slot, :count, :]) + mm(
                    q_rope[:, :ROPE_DIM], rope[t, :, :count]
                )

        def weigh(group, count):
            for j in range(SEQ_STEP):
                slot = group * SEQ_STEP + j
                sum_s[slot] = mm(prob_s[slot, :, :count].astype(BF16), latent[slot, :count, :])

        def score_step(group, carry):
            @pl.when(group + GROUPS_AHEAD < group_count)
            def _():
                cache_start(group + GROUPS_AHEAD)

            @pl.when(group == 0)
            def _():
                weight_copy(5).start()
                weight_copy(6).start()

            @pl.when(group == group_count - 1)
            def _():
                for i in range(7, weight_count):
                    weight_copy(i).start()

            for_blocks(group, score)
            return carry

        def weigh_step(group, carry):
            for_blocks(group, weigh)
            return carry

        rope_copy.wait()
        lax.fori_loop(0, group_count, score_step, 0)

        position = lax.broadcasted_iota(jnp.int32, (HEADS, n_pos), 1)
        ends = []
        for slot in range(n_seq):
            t = order_s[slot]
            own_row = latent_row_s[pl.ds(t, 1), :]
            own_key = key_row_s[pl.ds(t, 1), :]
            own = (
                jnp.sum(q_lat_s[t].astype(BF16).astype(F32) * own_row, axis=1, keepdims=True)
                + jnp.sum(q_rope_s[t].astype(BF16).astype(F32) * own_key, axis=1, keepdims=True)
            ) * scale
            scores = jnp.where(position < len_ref[t], score_s[slot] * scale, -jnp.inf)
            peak = jnp.maximum(jnp.max(scores, axis=1, keepdims=True), own)
            probs = jnp.exp(scores - peak)
            own_prob = jnp.exp(own - peak)
            ends.append((own_prob, jnp.sum(probs, axis=1, keepdims=True) + own_prob))
            prob_s[slot] = probs

        lax.fori_loop(0, group_count, weigh_step, 0)

        for slot, (own_prob, total) in enumerate(ends):
            t = order_s[slot]
            own_row = latent_row_s[pl.ds(t, 1), :]
            summed = sum_s[slot] + own_prob.astype(BF16).astype(F32) * own_row
            o_lat_s[:, pl.ds(t, 1), :] = (summed / total)[:, None, :]

        weight_copy(5).wait()
        parts = []
        for head in range(HEADS):
            parts.append(
                mm(
                    o_lat_s[head].astype(BF16),
                    vup[:, head * VALUE_DIM : (head + 1) * VALUE_DIM],
                ).astype(BF16)
            )
        heads_out = jnp.concatenate(parts, axis=1)
        weight_copy(6).wait()
        for i in range(7, weight_count):
            weight_copy(i).wait()
        mixed = (tokens + mm(heads_out, w_out[...])).astype(BF16).astype(F32)
        mixed_ref[...] = mixed
        mixed_copy = pltpu.make_async_copy(mixed_ref, mixed_hbm, o_sem.at[1])
        mixed_copy.start()
        moe_in = norm_gain(mixed, moe_gain_ref[...])
        for side in range(2):
            for r in range(chunks):
                col = side * half + r * LANES
                rows_s[side, r * ROWS : r * ROWS + n_seq, :] = moe_in[:, col : col + LANES]
            out = mm(picked, rows_s[side].astype(BF16)).astype(BF16)
            send_ref[:, side] = out.reshape(shape3)
        combine_copy.wait()
        mixed_copy.wait()

    return body


def run_mixer(side, tokens, cache_latent, cache_rope, cache_lengths, ids, weights, gains, mats, experts, half_count):
    n_seq, width = tokens.shape
    _, n_pos, lat = cache_latent.shape
    expert_count = half_count // 2
    slot_count = capacity_of(half_count)
    half = width // 2
    hidden = experts[0].shape[1]
    chunks = half // LANES
    rows_per = slot_count * chunks
    vmem = pl.BlockSpec(memory_space=pltpu.VMEM)
    hbm = pl.BlockSpec(memory_space=pltpu.HBM)
    small = [
        cache_lengths,
        tokens,
        jnp.asarray(inverse_row()),
        ids.T,
        weights.T,
        *[g.reshape(1, -1) for g in gains],
    ]
    return pl.pallas_call(
        mixer(n_seq, n_pos, width, lat, expert_count, slot_count),
        out_shape=(
            pltpu.HBM((n_seq, width), F32),
            jax.ShapeDtypeStruct((n_seq, lat), BF16),
            jax.ShapeDtypeStruct((n_seq, ROPE_DIM), BF16),
            jax.ShapeDtypeStruct((expert_count, 2, rows_per, LANES), BF16),
            pltpu.HBM((2, LANES, expert_count * rows_per), BF16),
            jax.ShapeDtypeStruct((half, hidden), BF16),
            jax.ShapeDtypeStruct((half, hidden), BF16),
            jax.ShapeDtypeStruct((hidden, half), BF16),
            jax.ShapeDtypeStruct((3 * half, hidden), BF16),
        ),
        in_specs=[pl.BlockSpec(memory_space=pltpu.SMEM)] + [hbm] * (len(small) + len(mats) + 2 + len(experts)),
        out_specs=(hbm, vmem, vmem, vmem, hbm) + (vmem,) * 4,
        scratch_shapes=[pltpu.SMEM((n_seq,), jnp.int32)]
        + [pltpu.VMEM(m.shape, m.dtype) for m in small[1:]]
        + [
            pltpu.VMEM((n_seq, width), F32),
            pltpu.VMEM((2, LANES, expert_count * rows_per), BF16),
        ]
        + [pltpu.VMEM(m.shape, BF16) for m in mats]
        + [
            pltpu.VMEM((n_seq, n_pos, lat), BF16),
            pltpu.VMEM((n_seq, ROPE_DIM, n_pos), BF16),
            pltpu.SMEM((n_seq,), jnp.int32),
            pltpu.SMEM((n_seq,), jnp.int32),
            pltpu.VMEM((n_seq, HEADS, n_pos), F32),
            pltpu.VMEM((n_seq, HEADS, n_pos), F32),
            pltpu.VMEM((n_seq, HEADS, lat), F32),
            pltpu.VMEM((n_seq, HEADS, lat), F32),
            pltpu.VMEM((n_seq, HEADS, LANES), F32),
            pltpu.VMEM((HEADS, n_seq, lat), F32),
            pltpu.VMEM((2, chunks * ROWS, LANES), F32),
            pltpu.VMEM((n_seq, lat), F32),
            pltpu.VMEM((n_seq, LANES), F32),
            pltpu.SemaphoreType.DMA((12 + half // hidden,)),
            pltpu.SemaphoreType.DMA((n_seq,)),
            pltpu.SemaphoreType.DMA((1,)),
            pltpu.SemaphoreType.DMA((len(small),)),
            pltpu.SemaphoreType.DMA((2,)),
        ],
        compiler_params=pltpu.CompilerParams(vmem_limit_bytes=44 * 1024 * 1024),
        name="mixer",
    )(
        side,
        *[
            pltpu.with_memory_space_constraint(m, pltpu.HBM)
            for m in (*small, *mats, cache_latent, jnp.swapaxes(cache_rope, 1, 2), *experts)
        ],
    )


def inner_kernel(rows, chunks, hidden):
    half = chunks * LANES

    def body(own_ref, gate_ref, up_ref, other_ref, keep_ref, give_ref, wide):
        wide[...] = own_ref[...].astype(F32)
        cols = [wide[pl.ds(r, rows, stride=chunks), :].astype(BF16) for r in range(chunks)]
        own = jnp.concatenate(cols, axis=1)
        mats = (gate_ref[...], up_ref[...], other_ref[:half, :], other_ref[half : 2 * half, :])
        for i, mat in enumerate(mats):
            part = mm(own, mat)
            keep_ref[:, i * hidden : (i + 1) * hidden] = part
            place = (i + 2) % 4
            give_ref[:, place * hidden : (place + 1) * hidden] = part.astype(BF16)

    return body


def run_inner(own, gate, up, other):
    count, _ = own.shape
    half, hidden = gate.shape
    chunks = half // LANES
    rows = count // chunks
    vmem = pl.BlockSpec(memory_space=pltpu.VMEM)
    return pl.pallas_call(
        inner_kernel(rows, chunks, hidden),
        out_shape=(
            jax.ShapeDtypeStruct((rows, 4 * hidden), F32),
            jax.ShapeDtypeStruct((rows, 4 * hidden), BF16),
        ),
        in_specs=[vmem] * 4,
        out_specs=(vmem, vmem),
        scratch_shapes=[pltpu.VMEM((count, LANES), F32)],
        compiler_params=pltpu.CompilerParams(vmem_limit_bytes=12 * 1024 * 1024),
        name="expert_inner",
    )(own, gate, up, other)


def outer_kernel(rows, chunks, hidden):
    half = chunks * LANES

    def body(keep_ref, given_ref, down_ref, other_ref, out_ref, wide):
        total = keep_ref[...] + given_ref[...].astype(F32)
        acts = []
        for start in (0, 2 * hidden):
            gate = total[:, start : start + hidden]
            up = total[:, start + hidden : start + 2 * hidden]
            acts.append((gate * jax.nn.sigmoid(gate) * up).astype(BF16))
        for b in range(half // hidden):
            cols = slice(b * hidden, (b + 1) * hidden)
            base = 2 * half + b * hidden
            out = mm(acts[0], down_ref[:, cols]) + mm(acts[1], other_ref[base : base + hidden, :])
            for r in range(hidden // LANES):
                row = b * (hidden // LANES) + r
                wide[pl.ds(row, rows, stride=chunks), :] = out[:, r * LANES : (r + 1) * LANES]
        out_ref[...] = wide[...].astype(BF16)

    return body


def run_outer(keep, given, down, other):
    rows, _ = keep.shape
    hidden, half = down.shape
    chunks = half // LANES
    vmem = pl.BlockSpec(memory_space=pltpu.VMEM)
    return pl.pallas_call(
        outer_kernel(rows, chunks, hidden),
        out_shape=jax.ShapeDtypeStruct((rows * chunks, LANES), BF16),
        in_specs=[vmem] * 4,
        out_specs=vmem,
        scratch_shapes=[pltpu.VMEM((rows * chunks, LANES), F32)],
        compiler_params=pltpu.CompilerParams(vmem_limit_bytes=12 * 1024 * 1024),
        name="expert_outer",
    )(keep, given, down, other)


def combine_kernel(n_seq, chunks):
    half = chunks * LANES

    def body(mixed_ref, combine_ref, rows_ref, out_ref):
        expert_count, _, rows_per, _ = rows_ref.shape
        combine = combine_ref[...].reshape(2 * LANES, expert_count * rows_per)
        for side in range(2):
            rows = rows_ref[:, side].reshape(expert_count * rows_per, LANES)
            both = mm(combine, rows)
            total = both[:LANES] + both[LANES:]
            for r in range(chunks):
                col = slice(side * half + r * LANES, side * half + (r + 1) * LANES)
                out_ref[:, col] = mixed_ref[:, col] + total[r * ROWS : r * ROWS + n_seq, :]

    return body


def run_combine(mixed, combine, rows):
    n_seq, width = mixed.shape
    vmem = pl.BlockSpec(memory_space=pltpu.VMEM)
    return pl.pallas_call(
        combine_kernel(n_seq, width // 2 // LANES),
        out_shape=jax.ShapeDtypeStruct(mixed.shape, F32),
        in_specs=[vmem] * 3,
        out_specs=vmem,
        compiler_params=pltpu.CompilerParams(vmem_limit_bytes=12 * 1024 * 1024),
        name="combine",
    )(mixed, combine, rows)


def shards(
    tokens,
    cache_latent,
    cache_rope,
    cache_lengths,
    expert_ids,
    route_weight,
    attn_gain,
    q_gain,
    kv_gain,
    moe_gain,
    w_qdown,
    w_kvdown,
    w_krope,
    w_qup,
    w_kup,
    w_vup,
    w_out,
    expert_gate,
    expert_up,
    expert_down,
):
    half_count = lax.axis_size("ep")
    side = jnp.bitwise_and(lax.axis_index("ep"), 1).reshape(1)
    mixed_attn, new_latent, new_rope_key, send, combine, gate, up, down, give = run_mixer(
        side,
        tokens,
        cache_latent,
        cache_rope,
        cache_lengths,
        expert_ids,
        route_weight,
        (attn_gain, q_gain, kv_gain, moe_gain),
        (w_qdown, w_kvdown, w_krope.T, w_qup, w_kup, w_vup, w_out),
        (expert_gate[0], expert_up[0], expert_down[0]),
        half_count,
    )
    block = send.shape[2]
    other = partner(give, "ep", 0)
    own = lax.all_to_all(
        send.reshape(half_count, block, LANES), "ep", split_axis=0, concat_axis=0, tiled=True
    )
    keep, inner = run_inner(own.reshape(half_count * block, LANES), gate, up, other)
    outputs = run_outer(keep, partner(inner, "ep", 0), down, other)
    returned = lax.all_to_all(
        outputs.reshape(half_count, block, LANES), "ep", split_axis=0, concat_axis=0, tiled=True
    )
    mixed = run_combine(mixed_attn, combine, returned.reshape(half_count // 2, 2, block, LANES))
    return (mixed, new_latent, new_rope_key)


def solution(mesh):
    placed = (
        P("ep", None),
        P("ep", None, None),
        P("ep", None, None),
        P("ep"),
        P("ep", None),
        P("ep", None),
        P(),
        P(),
        P(),
        P(),
        P(),
        P(),
        P(),
        P(),
        P(),
        P(),
        P(),
        P("ep", None, None),
        P("ep", None, None),
        P("ep", None, None),
    )
    return jax.shard_map(
        shards,
        mesh=mesh,
        in_specs=placed,
        out_specs=(P("ep", None), P("ep", None), P("ep", None)),
        check_vma=False,
    )
```

```python
import jax
import jax.numpy as jnp
import numpy as np
from jax import lax
from jax.experimental import pallas as pl
from jax.experimental.pallas import tpu as pltpu
from jax.sharding import PartitionSpec as P

HEADS = 8
NOPE_DIM = 128
ROPE_DIM = 64
VALUE_DIM = 128
GROUP_SIZE = 16
TOP_K = 6
SEQ_DEV = 12
LANES = 128
ROWS = 16
SEQ_STEP = 3
GROUPS_AHEAD = 4
BLOCK_POS = 128

EPS = 1e-06
THETA = 10000.0
F32 = jnp.float32
BF16 = jnp.bfloat16


def mm(a, b):
    return jnp.dot(a, b, preferred_element_type=F32)


def mm_t(a, b):
    return lax.dot_general(a, b, (((1,), (1,)), ((), ())), preferred_element_type=F32)


def partner(value, axis, bit):
    mask = 2**bit
    pairs = [(source, source ^ mask) for source in range(lax.axis_size(axis))]
    return lax.ppermute(value, axis, pairs)


def norm_gain(values, gain_vec):
    return values * lax.rsqrt(jnp.mean(values * values, axis=-1, keepdims=True) + EPS) * gain_vec


def capacity_of(half_count):
    group_count = half_count // 2 // GROUP_SIZE
    group_most = min(SEQ_DEV, max(3, 2 * ((SEQ_DEV + group_count - 1) // group_count)))
    return (TOP_K * group_most + GROUP_SIZE - 1) // GROUP_SIZE


def inverse_row():
    half_width = ROPE_DIM // 2
    inverse = THETA ** (-np.arange(half_width) / half_width)
    return np.tile(inverse, LANES // half_width).reshape(1, LANES).astype(np.float32)


def mixer(n_seq, n_pos, width, lat, expert_count, slot_count):
    scale = (NOPE_DIM + ROPE_DIM) ** (-0.5)
    half = width // 2
    chunks = half // LANES

    def body(
        side_ref,
        len_hbm,
        tokens_hbm,
        inverse_hbm,
        ids_hbm,
        weight_hbm,
        attn_gain_hbm,
        q_gain_hbm,
        kv_gain_hbm,
        moe_gain_hbm,
        qdown_hbm,
        kvdown_hbm,
        krope_hbm,
        qup_hbm,
        kup_hbm,
        vup_hbm,
        out_hbm,
        latent_hbm,
        rope_hbm,
        gate_hbm,
        up_hbm,
        down_hbm,
        mixed_hbm,
        new_latent_ref,
        new_rope_ref,
        send_ref,
        combine_hbm,
        gate_ref,
        up_ref,
        down_ref,
        give_ref,
        len_ref,
        tokens_ref,
        inverse_ref,
        ids_ref,
        weight_ref,
        attn_gain_ref,
        q_gain_ref,
        kv_gain_ref,
        moe_gain_ref,
        mixed_ref,
        combine_ref,
        qdown,
        kvdown,
        krope,
        qup,
        kup,
        vup,
        w_out,
        latent,
        rope,
        order_s,
        blocks_s,
        score_s,
        prob_s,
        sum_s,
        q_lat_s,
        q_rope_s,
        o_lat_s,
        rows_s,
        latent_row_s,
        key_row_s,
        w_sem,
        c_sem,
        r_sem,
        s_sem,
        o_sem,
    ):
        side = side_ref[0]
        hidden = gate_hbm.shape[1]
        here = pl.ds(pl.multiple_of(side * half, half), half)
        there = pl.ds(pl.multiple_of((1 - side) * half, half), half)
        weight_count = 12 + half // hidden
        small = [
            pltpu.make_async_copy(source, target, s_sem.at[i])
            for i, (source, target) in enumerate(
                (
                    (tokens_hbm, tokens_ref),
                    (attn_gain_hbm, attn_gain_ref),
                    (len_hbm, len_ref),
                    (inverse_hbm, inverse_ref),
                    (ids_hbm, ids_ref),
                    (weight_hbm, weight_ref),
                    (q_gain_hbm, q_gain_ref),
                    (kv_gain_hbm, kv_gain_ref),
                    (moe_gain_hbm, moe_gain_ref),
                )
            )
        ]
        for copy in small:
            copy.start()

        def weight_copy(i):
            pairs = [
                (qdown_hbm, qdown),
                (kvdown_hbm, kvdown),
                (krope_hbm, krope),
                (qup_hbm, qup),
                (kup_hbm, kup),
                (vup_hbm, vup),
                (out_hbm, w_out),
                (gate_hbm.at[here, :], gate_ref),
                (up_hbm.at[here, :], up_ref),
                (down_hbm.at[:, here], down_ref),
                (gate_hbm.at[there, :], give_ref.at[:half, :]),
                (up_hbm.at[there, :], give_ref.at[half : 2 * half, :]),
            ]
            for b in range(half // hidden):
                cols = slice(b * hidden, (b + 1) * hidden)
                rows = slice(2 * half + b * hidden, 2 * half + (b + 1) * hidden)
                pairs.append((down_hbm.at[:, there].at[:, cols], give_ref.at[rows, :]))
            return pltpu.make_async_copy(pairs[i][0], pairs[i][1], w_sem.at[i])

        group_count = n_seq // SEQ_STEP
        most_blocks = pl.cdiv(n_pos, BLOCK_POS)

        def for_blocks(group, act):
            for block in range(most_blocks):

                @pl.when(blocks_s[group] == block + 1)
                def _(count=min(n_pos, (block + 1) * BLOCK_POS)):
                    act(group, count)

        def latent_copies(group, count):
            slots = [group * SEQ_STEP + j for j in range(SEQ_STEP)]
            return [
                pltpu.make_async_copy(
                    latent_hbm.at[order_s[slot], :count, :],
                    latent.at[slot, :count, :],
                    c_sem.at[slot],
                )
                for slot in slots
            ]

        def start_all(group, count):
            for copy in latent_copies(group, count):
                copy.start()

        def cache_start(group):
            for_blocks(group, start_all)

        rope_copy = pltpu.make_async_copy(rope_hbm, rope, r_sem.at[0])

        weight_copy(0).start()
        weight_copy(1).start()

        small[2].wait()
        lengths = [len_ref[t] for t in range(n_seq)]
        places = [jnp.int32(0)] * n_seq
        for i in range(n_seq):
            for j in range(i):
                later = (lengths[i] > lengths[j]).astype(jnp.int32)
                places[j] = places[j] + later
                places[i] = places[i] + (1 - later)
        for t in range(n_seq):
            order_s[places[t]] = jnp.int32(t)
        for group in range(group_count):
            longest = len_ref[order_s[group * SEQ_STEP]]
            blocks_s[group] = (longest + (BLOCK_POS - 1)) // BLOCK_POS

        expert_row = lax.broadcasted_iota(jnp.int32, (expert_count, LANES), 0)
        for i, copy in enumerate(small):
            if i != 2:
                copy.wait()
        token_lane = lax.broadcasted_iota(jnp.int32, (n_seq, LANES), 1)
        token_row = lax.broadcasted_iota(jnp.int32, (n_seq, LANES), 0)
        spread = (token_lane % ROWS == token_row).astype(BF16)
        valid = lax.broadcasted_iota(jnp.int32, (TOP_K, LANES), 1) % ROWS < n_seq
        ids = jnp.where(valid, mm(ids_ref[...].astype(F32).astype(BF16), spread), -1.0)
        ids = ids.astype(jnp.int32)
        weight = weight_ref[...]
        weight_high = weight.astype(BF16)
        weight_low = mm((weight - weight_high.astype(F32)).astype(BF16), spread)
        weight_high = mm(weight_high, spread)
        taken = jnp.zeros((expert_count, LANES), F32)
        share_high = jnp.zeros((expert_count, LANES), F32)
        share_low = jnp.zeros((expert_count, LANES), F32)
        for k in range(TOP_K):
            hit = ids[k : k + 1, :] == expert_row
            taken = jnp.where(hit, 1.0, taken)
            share_high = jnp.where(hit, weight_high[k : k + 1, :], share_high)
            share_low = jnp.where(hit, weight_low[k : k + 1, :], share_low)
        for i in range(2, 5):
            weight_copy(i).start()
        row_a = lax.broadcasted_iota(jnp.int32, (LANES, LANES), 0)
        row_b = lax.broadcasted_iota(jnp.int32, (LANES, LANES), 1)
        before = ((row_a // ROWS == row_b // ROWS) & (row_a < row_b)).astype(BF16)
        rank = mm(taken.astype(BF16), before)
        rank = jnp.where(taken > 0.5, rank, -1.0)
        rows_per = slot_count * chunks
        shape3 = (expert_count, rows_per, LANES)
        sub = lax.broadcasted_iota(jnp.int32, shape3, 1)
        lane3 = lax.broadcasted_iota(jnp.int32, shape3, 2)
        placed = (rank[:, None, :] == (sub // chunks).astype(F32)) & (sub % chunks == lane3 // ROWS)
        flat = (expert_count * rows_per, LANES)
        picked = jnp.where(placed, 1.0, 0.0).reshape(flat).astype(BF16)
        for part, share in ((0, share_high), (1, share_low)):
            back = jnp.where(placed, jnp.broadcast_to(share[:, None, :], shape3), 0.0)
            combine_ref[part] = back.reshape(flat).T.astype(BF16)
        combine_copy = pltpu.make_async_copy(combine_ref, combine_hbm, o_sem.at[0])
        combine_copy.start()
        rows_s[...] = jnp.zeros_like(rows_s)

        tokens = tokens_ref[...].astype(F32)
        normed = norm_gain(tokens, attn_gain_ref[...]).astype(BF16)
        weight_copy(0).wait()
        rope_copy.start()
        cache_start(0)
        q_low = norm_gain(mm(normed, qdown[...]), q_gain_ref[...]).astype(BF16)
        weight_copy(1).wait()
        cache_start(1)
        new_latent = norm_gain(mm(normed, kvdown[...]), kv_gain_ref[...]).astype(BF16)
        new_latent_ref[...] = new_latent
        latent_row_s[...] = new_latent.astype(F32)
        weight_copy(2).wait()
        key_raw = mm_t(normed, krope[...])
        low_half = lax.broadcasted_iota(jnp.int32, (n_seq, LANES), 1)
        first_quarter = low_half % ROPE_DIM < ROPE_DIM // 2
        low_half = low_half < ROPE_DIM

        length = jnp.zeros((n_seq, LANES), F32)
        for t in range(n_seq):
            length = jnp.where(token_row == t, len_ref[t].astype(F32), length)
        angle = length * inverse_ref[...]
        cosine = jnp.cos(angle)
        sine = jnp.sin(angle)
        sine = jnp.where(first_quarter, -sine, sine)

        def rotate(v):
            swapped = jnp.where(
                first_quarter,
                pltpu.roll(v, LANES - ROPE_DIM // 2, 1),
                pltpu.roll(v, ROPE_DIM // 2, 1),
            )
            return v * cosine + swapped * sine

        new_key = rotate(jnp.concatenate([key_raw, key_raw], axis=1))
        new_key = new_key.astype(BF16)
        new_rope_ref[...] = new_key[:, :ROPE_DIM]
        key_row_s[...] = jnp.where(low_half, new_key.astype(F32), 0.0)

        weight_copy(3).wait()
        for group in range(2, GROUPS_AHEAD):
            cache_start(group)
        query = mm(q_low, qup[...])
        weight_copy(4).wait()
        for pair in range(HEADS // 2):
            base = 3 * LANES * pair
            first = query[:, base : base + LANES]
            middle = query[:, base + LANES : base + 2 * LANES]
            last = query[:, base + 2 * LANES : base + 3 * LANES]
            second = jnp.where(
                low_half, pltpu.roll(middle, ROPE_DIM, 1), pltpu.roll(last, ROPE_DIM, 1)
            )
            both = rotate(jnp.where(low_half, middle, last))
            for side, nope in ((0, first), (1, second)):
                head = 2 * pair + side
                q_lat_s[:, head, :] = mm_t(
                    nope.astype(BF16), kup[:, head * NOPE_DIM : (head + 1) * NOPE_DIM]
                )
                turned = both if side == 0 else pltpu.roll(both, ROPE_DIM, 1)
                q_rope_s[:, head, :] = turned

        def score(group, count):
            for copy in latent_copies(group, count):
                copy.wait()
            for j in range(SEQ_STEP):
                slot = group * SEQ_STEP + j
                t = order_s[slot]
                q_lat = q_lat_s[t].astype(BF16)
                q_rope = q_rope_s[t].astype(BF16)
                score_s[slot, :, :count] = mm_t(q_lat, latent[slot, :count, :]) + mm(
                    q_rope[:, :ROPE_DIM], rope[t, :, :count]
                )

        def weigh(group, count):
            for j in range(SEQ_STEP):
                slot = group * SEQ_STEP + j
                sum_s[slot] = mm(prob_s[slot, :, :count].astype(BF16), latent[slot, :count, :])

        def score_step(group, carry):
            @pl.when(group + GROUPS_AHEAD < group_count)
            def _():
                cache_start(group + GROUPS_AHEAD)

            @pl.when(group == 0)
            def _():
                weight_copy(5).start()
                weight_copy(6).start()

            @pl.when(group == group_count - 1)
            def _():
                for i in range(7, weight_count):
                    weight_copy(i).start()

            for_blocks(group, score)
            return carry

        def weigh_step(group, carry):
            for_blocks(group, weigh)
            return carry

        rope_copy.wait()
        lax.fori_loop(0, group_count, score_step, 0)

        position = lax.broadcasted_iota(jnp.int32, (HEADS, n_pos), 1)
        ends = []
        for slot in range(n_seq):
            t = order_s[slot]
            own_row = latent_row_s[pl.ds(t, 1), :]
            own_key = key_row_s[pl.ds(t, 1), :]
            own = (
                jnp.sum(q_lat_s[t].astype(BF16).astype(F32) * own_row, axis=1, keepdims=True)
                + jnp.sum(q_rope_s[t].astype(BF16).astype(F32) * own_key, axis=1, keepdims=True)
            ) * scale
            scores = jnp.where(position < len_ref[t], score_s[slot] * scale, -jnp.inf)
            peak = jnp.maximum(jnp.max(scores, axis=1, keepdims=True), own)
            probs = jnp.exp(scores - peak)
            own_prob = jnp.exp(own - peak)
            ends.append((own_prob, jnp.sum(probs, axis=1, keepdims=True) + own_prob))
            prob_s[slot] = probs

        lax.fori_loop(0, group_count, weigh_step, 0)

        for slot, (own_prob, total) in enumerate(ends):
            t = order_s[slot]
            own_row = latent_row_s[pl.ds(t, 1), :]
            summed = sum_s[slot] + own_prob.astype(BF16).astype(F32) * own_row
            o_lat_s[:, pl.ds(t, 1), :] = (summed / total)[:, None, :]

        weight_copy(5).wait()
        parts = []
        for head in range(HEADS):
            parts.append(
                mm(
                    o_lat_s[head].astype(BF16),
                    vup[:, head * VALUE_DIM : (head + 1) * VALUE_DIM],
                ).astype(BF16)
            )
        heads_out = jnp.concatenate(parts, axis=1)
        weight_copy(6).wait()
        for i in range(7, weight_count):
            weight_copy(i).wait()
        mixed = (tokens + mm(heads_out, w_out[...])).astype(BF16).astype(F32)
        mixed_ref[...] = mixed
        mixed_copy = pltpu.make_async_copy(mixed_ref, mixed_hbm, o_sem.at[1])
        mixed_copy.start()
        moe_in = norm_gain(mixed, moe_gain_ref[...])
        for side in range(2):
            for r in range(chunks):
                col = side * half + r * LANES
                rows_s[side, r * ROWS : r * ROWS + n_seq, :] = moe_in[:, col : col + LANES]
            out = mm(picked, rows_s[side].astype(BF16)).astype(BF16)
            send_ref[:, side] = out.reshape(shape3)
        combine_copy.wait()
        mixed_copy.wait()

    return body


def run_mixer(side, tokens, cache_latent, cache_rope, cache_lengths, ids, weights, gains, mats, experts, half_count):
    n_seq, width = tokens.shape
    _, n_pos, lat = cache_latent.shape
    expert_count = half_count // 2
    slot_count = capacity_of(half_count)
    half = width // 2
    hidden = experts[0].shape[1]
    chunks = half // LANES
    rows_per = slot_count * chunks
    vmem = pl.BlockSpec(memory_space=pltpu.VMEM)
    hbm = pl.BlockSpec(memory_space=pltpu.HBM)
    small = [
        cache_lengths,
        tokens,
        jnp.asarray(inverse_row()),
        ids.T,
        weights.T,
        *[g.reshape(1, -1) for g in gains],
    ]
    return pl.pallas_call(
        mixer(n_seq, n_pos, width, lat, expert_count, slot_count),
        out_shape=(
            pltpu.HBM((n_seq, width), F32),
            jax.ShapeDtypeStruct((n_seq, lat), BF16),
            jax.ShapeDtypeStruct((n_seq, ROPE_DIM), BF16),
            jax.ShapeDtypeStruct((expert_count, 2, rows_per, LANES), BF16),
            pltpu.HBM((2, LANES, expert_count * rows_per), BF16),
            jax.ShapeDtypeStruct((half, hidden), BF16),
            jax.ShapeDtypeStruct((half, hidden), BF16),
            jax.ShapeDtypeStruct((hidden, half), BF16),
            jax.ShapeDtypeStruct((3 * half, hidden), BF16),
        ),
        in_specs=[pl.BlockSpec(memory_space=pltpu.SMEM)] + [hbm] * (len(small) + len(mats) + 2 + len(experts)),
        out_specs=(hbm, vmem, vmem, vmem, hbm) + (vmem,) * 4,
        scratch_shapes=[pltpu.SMEM((n_seq,), jnp.int32)]
        + [pltpu.VMEM(m.shape, m.dtype) for m in small[1:]]
        + [
            pltpu.VMEM((n_seq, width), F32),
            pltpu.VMEM((2, LANES, expert_count * rows_per), BF16),
        ]
        + [pltpu.VMEM(m.shape, BF16) for m in mats]
        + [
            pltpu.VMEM((n_seq, n_pos, lat), BF16),
            pltpu.VMEM((n_seq, ROPE_DIM, n_pos), BF16),
            pltpu.SMEM((n_seq,), jnp.int32),
            pltpu.SMEM((n_seq,), jnp.int32),
            pltpu.VMEM((n_seq, HEADS, n_pos), F32),
            pltpu.VMEM((n_seq, HEADS, n_pos), F32),
            pltpu.VMEM((n_seq, HEADS, lat), F32),
            pltpu.VMEM((n_seq, HEADS, lat), F32),
            pltpu.VMEM((n_seq, HEADS, LANES), F32),
            pltpu.VMEM((HEADS, n_seq, lat), F32),
            pltpu.VMEM((2, chunks * ROWS, LANES), F32),
            pltpu.VMEM((n_seq, lat), F32),
            pltpu.VMEM((n_seq, LANES), F32),
            pltpu.SemaphoreType.DMA((12 + half // hidden,)),
            pltpu.SemaphoreType.DMA((n_seq,)),
            pltpu.SemaphoreType.DMA((1,)),
            pltpu.SemaphoreType.DMA((len(small),)),
            pltpu.SemaphoreType.DMA((2,)),
        ],
        compiler_params=pltpu.CompilerParams(vmem_limit_bytes=44 * 1024 * 1024),
        name="mixer",
    )(
        side,
        *[
            pltpu.with_memory_space_constraint(m, pltpu.HBM)
            for m in (*small, *mats, cache_latent, jnp.swapaxes(cache_rope, 1, 2), *experts)
        ],
    )


def inner_kernel(rows, chunks, hidden):
    half = chunks * LANES

    def body(own_ref, gate_ref, up_ref, other_ref, keep_ref, give_ref, wide):
        wide[...] = own_ref[...].astype(F32)
        cols = [wide[pl.ds(r, rows, stride=chunks), :].astype(BF16) for r in range(chunks)]
        own = jnp.concatenate(cols, axis=1)
        mats = (gate_ref[...], up_ref[...], other_ref[:half, :], other_ref[half : 2 * half, :])
        for i, mat in enumerate(mats):
            part = mm(own, mat)
            keep_ref[:, i * hidden : (i + 1) * hidden] = part
            place = (i + 2) % 4
            give_ref[:, place * hidden : (place + 1) * hidden] = part.astype(BF16)

    return body


def run_inner(own, gate, up, other):
    count, _ = own.shape
    half, hidden = gate.shape
    chunks = half // LANES
    rows = count // chunks
    vmem = pl.BlockSpec(memory_space=pltpu.VMEM)
    return pl.pallas_call(
        inner_kernel(rows, chunks, hidden),
        out_shape=(
            jax.ShapeDtypeStruct((rows, 4 * hidden), F32),
            jax.ShapeDtypeStruct((rows, 4 * hidden), BF16),
        ),
        in_specs=[vmem] * 4,
        out_specs=(vmem, vmem),
        scratch_shapes=[pltpu.VMEM((count, LANES), F32)],
        compiler_params=pltpu.CompilerParams(vmem_limit_bytes=12 * 1024 * 1024),
        name="expert_inner",
    )(own, gate, up, other)


def outer_kernel(rows, chunks, hidden):
    half = chunks * LANES

    def body(keep_ref, given_ref, down_ref, other_ref, out_ref, wide):
        total = keep_ref[...] + given_ref[...].astype(F32)
        acts = []
        for start in (0, 2 * hidden):
            gate = total[:, start : start + hidden]
            up = total[:, start + hidden : start + 2 * hidden]
            acts.append((gate * jax.nn.sigmoid(gate) * up).astype(BF16))
        for b in range(half // hidden):
            cols = slice(b * hidden, (b + 1) * hidden)
            base = 2 * half + b * hidden
            out = mm(acts[0], down_ref[:, cols]) + mm(acts[1], other_ref[base : base + hidden, :])
            for r in range(hidden // LANES):
                row = b * (hidden // LANES) + r
                wide[pl.ds(row, rows, stride=chunks), :] = out[:, r * LANES : (r + 1) * LANES]
        out_ref[...] = wide[...].astype(BF16)

    return body


def run_outer(keep, given, down, other):
    rows, _ = keep.shape
    hidden, half = down.shape
    chunks = half // LANES
    vmem = pl.BlockSpec(memory_space=pltpu.VMEM)
    return pl.pallas_call(
        outer_kernel(rows, chunks, hidden),
        out_shape=jax.ShapeDtypeStruct((rows * chunks, LANES), BF16),
        in_specs=[vmem] * 4,
        out_specs=vmem,
        scratch_shapes=[pltpu.VMEM((rows * chunks, LANES), F32)],
        compiler_params=pltpu.CompilerParams(vmem_limit_bytes=12 * 1024 * 1024),
        name="expert_outer",
    )(keep, given, down, other)


def combine_kernel(n_seq, chunks):
    half = chunks * LANES

    def body(mixed_ref, combine_ref, rows_ref, out_ref):
        expert_count, _, rows_per, _ = rows_ref.shape
        combine = combine_ref[...].reshape(2 * LANES, expert_count * rows_per)
        for side in range(2):
            rows = rows_ref[:, side].reshape(expert_count * rows_per, LANES)
            both = mm(combine, rows)
            total = both[:LANES] + both[LANES:]
            for r in range(chunks):
                col = slice(side * half + r * LANES, side * half + (r + 1) * LANES)
                out_ref[:, col] = mixed_ref[:, col] + total[r * ROWS : r * ROWS + n_seq, :]

    return body


def run_combine(mixed, combine, rows):
    n_seq, width = mixed.shape
    vmem = pl.BlockSpec(memory_space=pltpu.VMEM)
    return pl.pallas_call(
        combine_kernel(n_seq, width // 2 // LANES),
        out_shape=jax.ShapeDtypeStruct(mixed.shape, F32),
        in_specs=[vmem] * 3,
        out_specs=vmem,
        compiler_params=pltpu.CompilerParams(vmem_limit_bytes=12 * 1024 * 1024),
        name="combine",
    )(mixed, combine, rows)


def shards(
    tokens,
    cache_latent,
    cache_rope,
    cache_lengths,
    expert_ids,
    route_weight,
    attn_gain,
    q_gain,
    kv_gain,
    moe_gain,
    w_qdown,
    w_kvdown,
    w_krope,
    w_qup,
    w_kup,
    w_vup,
    w_out,
    expert_gate,
    expert_up,
    expert_down,
):
    half_count = lax.axis_size("ep")
    side = jnp.bitwise_and(lax.axis_index("ep"), 1).reshape(1)
    mixed_attn, new_latent, new_rope_key, send, combine, gate, up, down, give = run_mixer(
        side,
        tokens,
        cache_latent,
        cache_rope,
        cache_lengths,
        expert_ids,
        route_weight,
        (attn_gain, q_gain, kv_gain, moe_gain),
        (w_qdown, w_kvdown, w_krope.T, w_qup, w_kup, w_vup, w_out),
        (expert_gate[0], expert_up[0], expert_down[0]),
        half_count,
    )
    block = send.shape[2]
    other = partner(give, "ep", 0)
    own = lax.all_to_all(
        send.reshape(half_count, block, LANES), "ep", split_axis=0, concat_axis=0, tiled=True
    )
    keep, inner = run_inner(own.reshape(half_count * block, LANES), gate, up, other)
    outputs = run_outer(keep, partner(inner, "ep", 0), down, other)
    returned = lax.all_to_all(
        outputs.reshape(half_count, block, LANES), "ep", split_axis=0, concat_axis=0, tiled=True
    )
    mixed = run_combine(mixed_attn, combine, returned.reshape(half_count // 2, 2, block, LANES))
    return (mixed, new_latent, new_rope_key)


def solution(mesh):
    placed = (
        P("ep", None),
        P("ep", None, None),
        P("ep", None, None),
        P("ep"),
        P("ep", None),
        P("ep", None),
        P(),
        P(),
        P(),
        P(),
        P(),
        P(),
        P(),
        P(),
        P(),
        P(),
        P(),
        P("ep", None, None),
        P("ep", None, None),
        P("ep", None, None),
    )
    return jax.shard_map(
        shards,
        mesh=mesh,
        in_specs=placed,
        out_specs=(P("ep", None), P("ep", None), P("ep", None)),
        check_vma=False,
    )
```
